512 devices in a mesh: kv: 32 (over z, core), tp: 16 (over y, x).
Axes of the slice: x: 4, y: 4, z: 16, core: 2. Of those that a mesh axis runs over, the one named last changes fastest.
Arguments:
- tokens: bfloat16 [24, 4096], P(None, 'kv'), may hold values from -24 to 24
- attention_norm_gain: float32 [4096], replicated, may hold values from 0.1 to 1.9
- query_weight: bfloat16 [4096, 2048], P('kv', 'tp'), may hold values from -0.09375 to 0.09375
- key_weight: bfloat16 [4096, 2048], P('kv', 'tp'), may hold values from -0.09375 to 0.09375
- value_weight: bfloat16 [4096, 4096], P('kv', 'tp'), may hold values from -0.09375 to 0.09375
- output_gate_weight: bfloat16 [4096, 4096], P('kv', 'tp'), may hold values from -0.09375 to 0.09375
- lowrank_weight: bfloat16 [4096, 16], replicated, may hold values from -0.09375 to 0.09375
- decay_weight: bfloat16 [16, 2048], replicated, may hold values from -1.5 to 1.5
- decay_preact_bias: float32 [2048], replicated, may hold values from -1 to 20
- head_norm_gain: float32 [256], replicated, may hold values from 0.1 to 1.9
- output_weight: bfloat16 [4096, 4096], P('tp', 'kv'), may hold values from -0.1875 to 0.1875
- feedforward_norm_gain: float32 [4096], replicated, may hold values from 0.1 to 1.9
- feedforward_gate_weight: bfloat16 [4096, 10240], P('kv', 'tp'), may hold values from -0.09375 to 0.09375
- feedforward_up_weight: bfloat16 [4096, 10240], P('kv', 'tp'), may hold values from -0.09375 to 0.09375
- feedforward_down_weight: bfloat16 [10240, 4096], P('tp', 'kv'), may hold values from -0.109375 to 0.109375
- past_key_cache: bfloat16 [24, 6144, 2048], P(None, 'kv', 'tp'), may hold values from -6 to 6
- past_value_cache: bfloat16 [24, 6144, 4096], P(None, 'kv', 'tp'), may hold values from -6 to 6
- past_lowrank_cache: bfloat16 [24, 16, 6144], P(None, None, 'kv'), may hold values from -8 to 8
- head_extra_decay: float32 [24, 16, 6144], P(None, 'tp', 'kv'), may hold values from -0.7 to 0
- lengths: int32 [24], replicated, may hold values from 1 to 6144, 41472 in all
Outputs:
- output: bfloat16 [24, 4096], P(None, 'kv')
The draws below stay inside these ranges and needn't reach their ends.
All inputs are finite; a program needn't handle non-finite values.
Results may differ from the reference program's by a relative error of at most 0.0085.
Values may be sent and summed in bfloat16 or wider, within the bound.
No kernel may reach another device: no remote copies, remote signals or barrier semaphores. Data moves between devices by JAX's collectives and lax.ppermute only.
A program may use at most 64 MiB of HBM per device.

```python
import math
import jax
import jax.numpy as jnp
import numpy as np
from jax import lax

D = 4096
HEADS = 16
KEY_CHANNELS = 128
DV = 256
RANK = 16
FF = 10240
SEQS = 24
POS_DEV = 192
LENGTH = 6144
KEYDIM = 2048
VALDIM = 4096


def draw_tokens(key, part):
    key_base, key_rows = jax.random.split(jax.random.fold_in(key, 11))
    columns = jnp.arange(D, dtype=jnp.float32) / D
    standard = jax.random.normal(key_base, (SEQS, D), jnp.float32)
    col_scale = 0.32 * 10.0 ** columns
    row_scale = jnp.exp(jax.random.uniform(key_rows, (SEQS, 1), jnp.float32, -1.15, 1.15))
    return jnp.clip(standard * col_scale[None, :] * row_scale, -24.0, 24.0).astype(jnp.bfloat16)


def draw_decay_preact_bias(key, part):
    key_pick, key_fast, key_slow = jax.random.split(jax.random.fold_in(key, 23), 3)
    order = jax.random.permutation(key_pick, HEADS)
    fast_value = jax.random.uniform(key_fast, (HEADS, KEY_CHANNELS), jnp.float32, -1.0, 0.5)
    fast_head = order < HEADS // 2
    slow_value = jnp.log(LENGTH * 1.0) + jax.random.uniform(key_slow, (HEADS, KEY_CHANNELS), jnp.float32, 1.0, 3.0)
    return jnp.where(fast_head[:, None], fast_value, slow_value).reshape(HEADS * KEY_CHANNELS).astype(jnp.float32)


def draw_past_lowrank_cache(key, part):
    key_value, key_scale = jax.random.split(jax.random.fold_in(key, 37))
    groups = LENGTH // POS_DEV
    standard = jax.random.normal(key_value, (SEQS, RANK, groups, POS_DEV), jnp.float32)
    group_scale = jnp.exp(jax.random.uniform(key_scale, (SEQS, 1, groups, 1), jnp.float32, -0.7, 0.7))
    return jnp.clip((standard * group_scale).reshape(SEQS, RANK, LENGTH), -8.0, 8.0).astype(jnp.bfloat16)


def draw_head_extra_decay(key, part):
    key_where, key_depth = jax.random.split(jax.random.fold_in(key, 41))
    array_shape = (SEQS, HEADS, LENGTH)
    struck = jax.random.uniform(key_where, array_shape, jnp.float32) < 4.0 / LENGTH
    kept = jax.random.uniform(key_depth, array_shape, jnp.float32, 0.5, 0.8)
    return jnp.where(struck, jnp.log(kept), 0.0).astype(jnp.float32)


def raised(entries, own_key, source, target, blocks, factor):
    def block_of(position):
        return (jnp.arange(entries.shape[position]) // (entries.shape[position] // blocks)).reshape((-1,) + (1,) * (entries.ndim - 1 - position))

    first = jax.random.permutation(own_key, blocks)[block_of(target)]
    second = (block_of(target) + blocks // 2) % blocks
    return jnp.where((block_of(source) == first) | (block_of(source) == second), factor * entries, entries)


def block_levels(stream_key, dims, cuts, low, high):
    gain, own = 1.0, jax.random.fold_in(stream_key, 6)
    for position, shards_of in cuts:
        draws = jnp.exp(jax.random.uniform(jax.random.fold_in(own, position), (shards_of,), jnp.float32, low / len(cuts), high / len(cuts)))
        gain = gain * jnp.repeat(draws, dims[position] // shards_of).reshape([-1 if axis == position else 1 for axis in range(len(dims))])
    return gain


def split_up(number_of, total, reach, skew):
    loads = [(1 << 20) // math.isqrt(standing ** skew) + 1 for standing in range(2, number_of + 1)]
    spare, given = total - reach - (number_of - 1), [1] * (number_of - 1)
    while spare > 0:
        movable = [i for i in range(number_of - 1) if given[i] < reach]
        whole, remaining = sum([loads[i] for i in movable]), spare
        for i in movable:
            more = min(reach - given[i], max(1, remaining * loads[i] // whole), spare)
            given[i] = given[i] + more
            spare = spare - more
    return np.array([reach] + given)


def uneven_parts(rng, number_of, total, reach, lean):
    if number_of == 2:
        one = jax.random.randint(rng, (), max(1, total - reach), min(reach, total - 1) + 1)
        return jnp.stack([one, total - one])
    sizes = jnp.asarray(split_up(number_of, total, reach, lean), jnp.int32)
    couples = (number_of - 1) // 2
    source_of, taker = sizes[1:1 + 2 * couples:2], sizes[2:2 + 2 * couples:2]
    room = jnp.minimum(source_of - 1, reach - taker)
    moved = jax.random.randint(jax.random.fold_in(rng, 1), (couples,), 0, 1 << 20) % (room + 1)
    sizes = sizes.at[1:1 + 2 * couples:2].set(source_of - moved).at[2:2 + 2 * couples:2].set(taker + moved)
    return sizes[jax.random.permutation(jax.random.fold_in(rng, 2), number_of)]


def scatter_about(rng, extent, width, reach, cuts=(), kind=jnp.bfloat16):
    level = block_levels(rng, extent, cuts, -0.22, 0.18) if cuts else 1.0
    array = jax.random.normal(rng, extent, jnp.float32) * width * level
    return jnp.minimum(jnp.maximum(array, -reach), reach).astype(kind)


def bell_draw_with(rng, extent, deviation, reach, shards, heavy, kind=jnp.bfloat16):
    values = deviation * jax.random.normal(rng, extent, jnp.float32)
    if shards:
        values = values * block_levels(rng, extent, shards, -0.22, 0.18)
    return jnp.clip(raised(values, jax.random.fold_in(rng, 3), *heavy), -reach, reach).astype(kind)


def setup_inputs(seed: int = 0) -> dict:
    arg_keys = jax.random.split(jax.random.key(seed), 21)
    return {
        "tokens": draw_tokens(jax.random.fold_in(arg_keys[20], 71), 0),
        "attention_norm_gain": jnp.clip(1.0 + 0.18 * jax.random.normal(arg_keys[1], (D,), jnp.float32), 0.1, 1.9),
        "query_weight": scatter_about(arg_keys[2], (D, KEYDIM), D ** -0.5, 0.09375, ((0, 32), (1, 16))),
        "key_weight": scatter_about(arg_keys[3], (D, KEYDIM), D ** -0.5, 0.09375, ((0, 32), (1, 16))),
        "value_weight": scatter_about(arg_keys[4], (D, VALDIM), D ** -0.5, 0.09375, ((0, 32), (1, 16))),
        "output_gate_weight": scatter_about(arg_keys[5], (D, VALDIM), D ** -0.5, 0.09375, ((0, 32), (1, 16))),
        "lowrank_weight": scatter_about(arg_keys[6], (D, RANK), D ** -0.5, 0.09375),
        "decay_weight": scatter_about(arg_keys[7], (RANK, KEYDIM), RANK ** -0.5, 1.5),
        "decay_preact_bias": draw_decay_preact_bias(jax.random.fold_in(arg_keys[20], 71), 0),
        "head_norm_gain": jnp.clip(1.0 + 0.18 * jax.random.normal(arg_keys[9], (DV,), jnp.float32), 0.1, 1.9),
        "output_weight": bell_draw_with(arg_keys[10], (VALDIM, D), VALDIM ** -0.5, 0.1875, ((0, 16), (1, 32)), (0, 1, 32, 2.75)),
        "feedforward_norm_gain": jnp.clip(1.0 + 0.18 * jax.random.normal(arg_keys[11], (D,), jnp.float32), 0.1, 1.9),
        "feedforward_gate_weight": scatter_about(arg_keys[12], (D, FF), D ** -0.5, 0.09375, ((0, 32), (1, 16))),
        "feedforward_up_weight": scatter_about(arg_keys[13], (D, FF), D ** -0.5, 0.09375, ((0, 32), (1, 16))),
        "feedforward_down_weight": bell_draw_with(arg_keys[14], (FF, D), FF ** -0.5, 0.109375, ((0, 16), (1, 32)), (0, 1, 32, 2.75)),
        "past_key_cache": scatter_about(arg_keys[15], (SEQS, LENGTH, KEYDIM), 1.0, 6.0, ((1, 32), (2, 16))),
        "past_value_cache": scatter_about(arg_keys[16], (SEQS, LENGTH, VALDIM), 1.0, 6.0, ((1, 32), (2, 16))),
        "past_lowrank_cache": draw_past_lowrank_cache(jax.random.fold_in(arg_keys[20], 71), 0),
        "head_extra_decay": draw_head_extra_decay(jax.random.fold_in(arg_keys[20], 71), 0),
        "lengths": uneven_parts(arg_keys[19], SEQS, (SEQS + 3) * LENGTH // 4, LENGTH, 2).astype(jnp.int32),
    }


NORM_EPSILON = 1e-06

def product(operand, weights):
    return jnp.dot(operand, weights, preferred_element_type=jnp.float32)

def reference(tokens, attention_norm_gain, query_weight, key_weight, value_weight, output_gate_weight, lowrank_weight, decay_weight, decay_preact_bias, head_norm_gain, output_weight, feedforward_norm_gain, feedforward_gate_weight, feedforward_up_weight, feedforward_down_weight, past_key_cache, past_value_cache, past_lowrank_cache, head_extra_decay, lengths):
    sequences = tokens.shape[0]
    rows_float = tokens.astype(jnp.float32)
    inv_rms = lax.rsqrt(lax.optimization_barrier(jnp.mean(rows_float * rows_float, axis=1, keepdims=True)) + NORM_EPSILON)
    scaled = (rows_float * attention_norm_gain).astype(jnp.bfloat16)
    query_vector = (inv_rms * product(scaled, query_weight)).astype(jnp.bfloat16)
    fresh_key = (inv_rms * product(scaled, key_weight)).astype(jnp.bfloat16)
    fresh_value = (inv_rms * product(scaled, value_weight)).astype(jnp.bfloat16)
    outgate = (inv_rms * product(scaled, output_gate_weight)).astype(jnp.bfloat16)
    lowrank = (inv_rms * product(scaled, lowrank_weight)).astype(jnp.bfloat16)
    fresh_gate_value = jax.nn.log_sigmoid(product(lowrank, decay_weight) + decay_preact_bias) / 16.0

    def single_sequence(layer_inputs):
        key_matrix, value_matrix, lowrank_inputs, extra_decays, valid_length, query_single, key_vector, value_vector, gate_vector = layer_inputs
        gate_preactivation = jnp.dot(lowrank_inputs.T, decay_weight, preferred_element_type=jnp.float32) + decay_preact_bias
        decay_gates = jax.nn.log_sigmoid(gate_preactivation) / 16.0 + jnp.repeat(extra_decays.T, KEY_CHANNELS, axis=1)
        is_live = jnp.arange(key_matrix.shape[0], dtype=jnp.int32) < valid_length
        decay_gates = jnp.where(is_live[:, None], decay_gates, 0.0)
        suffix = jnp.cumsum(decay_gates[::-1], axis=0)[::-1]
        exclusive = jnp.concatenate([suffix[1:], jnp.zeros((1, suffix.shape[1]), jnp.float32)], axis=0)
        weighting = jnp.exp(exclusive + gate_vector[None, :])
        query_scaled = query_single.astype(jnp.float32) * KEY_CHANNELS ** (-0.5)
        products = key_matrix.astype(jnp.float32) * weighting * query_scaled[None, :]
        scores = lax.optimization_barrier(jnp.sum(products.reshape(key_matrix.shape[0], HEADS, KEY_CHANNELS), axis=2))
        scores = jnp.where(is_live[:, None], scores, 0.0).astype(jnp.bfloat16)
        summed = jnp.einsum('lh,lhv->hv', scores.astype(jnp.float32), value_matrix.astype(jnp.float32).reshape(key_matrix.shape[0], HEADS, DV), precision=lax.Precision.HIGHEST)
        own_score = lax.optimization_barrier(jnp.sum((query_scaled * key_vector.astype(jnp.float32)).reshape(HEADS, KEY_CHANNELS), axis=1))
        return summed + own_score[:, None] * value_vector.astype(jnp.float32).reshape(HEADS, DV)
    mixer_output = lax.map(single_sequence, (past_key_cache, past_value_cache, past_lowrank_cache, head_extra_decay, lengths, query_vector, fresh_key, fresh_value, fresh_gate_value))
    mean_sq = lax.optimization_barrier(jnp.mean(mixer_output * mixer_output, axis=2, keepdims=True))
    gate_act = jax.nn.silu(outgate.astype(jnp.float32).reshape(sequences, HEADS, DV))
    gated = (mixer_output * lax.rsqrt(mean_sq + NORM_EPSILON) * head_norm_gain * gate_act).astype(jnp.bfloat16)
    residual = rows_float + product(gated.reshape(sequences, HEADS * DV), output_weight)
    inv_two = lax.rsqrt(lax.optimization_barrier(jnp.mean(residual * residual, axis=1, keepdims=True)) + NORM_EPSILON)
    scaled_two = (residual * feedforward_norm_gain).astype(jnp.bfloat16)
    hidden = (jax.nn.silu(inv_two * product(scaled_two, feedforward_gate_weight)) * (inv_two * product(scaled_two, feedforward_up_weight))).astype(jnp.bfloat16)
    return (residual + product(hidden, feedforward_down_weight)).astype(jnp.bfloat16)
```

```python
import jax
import jax.numpy as jnp
from jax import lax
from jax.sharding import Mesh
from jax.sharding import PartitionSpec as P

D = 4096
KEY_CHANNELS = 128
DV = 256
GROUPS = 8
MEMBERS = 4
OWN = 6
KV = ("kvh", "kvl")
TP = ("tp_0", "tp_1")
NORM_EPSILON = 1e-06
BF = jnp.bfloat16
F32 = jnp.float32


def exchange(array, axes):
    return lax.all_to_all(array, axes, split_axis=0, concat_axis=0, tiled=True)


def product(operand, weights):
    return jnp.dot(operand, weights, preferred_element_type=F32)


def copies(array, size):
    return jnp.broadcast_to(array, (size, *array.shape))


def split_two(array):
    high = array.astype(BF)
    low = (array - high.astype(F32)).astype(BF)
    return high.astype(F32), low.astype(F32)


def log_gate(values):
    return (jnp.minimum(values, 0.0) - jnp.log(1.0 + jnp.exp(-jnp.abs(values)))) / 16.0


def by_owner(rows):
    rest = rows.shape[1:]
    grid = jnp.swapaxes(rows.reshape(MEMBERS, OWN, *rest), 0, 1)
    pad = jnp.zeros((GROUPS - OWN, MEMBERS, *rest), rows.dtype)
    return jnp.concatenate([grid, pad]).reshape(GROUPS * MEMBERS, *rest)


def shards(
    tokens,
    attention_norm_gain,
    query_weight,
    key_weight,
    value_weight,
    output_gate_weight,
    lowrank_weight,
    decay_weight,
    decay_preact_bias,
    head_norm_gain,
    output_weight,
    feedforward_norm_gain,
    feedforward_gate_weight,
    feedforward_up_weight,
    feedforward_down_weight,
    past_key_cache,
    past_value_cache,
    past_lowrank_cache,
    head_extra_decay,
    lengths,
):
    sequences, width = tokens.shape
    group, member = lax.axis_index("kvh"), lax.axis_index("kvl")
    place = group * MEMBERS + member
    head = lax.axis_index(TP)
    positions = past_key_cache.shape[1]
    row_start = place * width
    tokens_f = tokens.astype(F32)
    gain_one = lax.dynamic_slice_in_dim(attention_norm_gain, row_start, width)
    scaled = (tokens_f * gain_one).astype(BF)
    low_rows = lax.dynamic_slice_in_dim(lowrank_weight, row_start, width, 0)
    squares = jnp.sum(tokens_f * tokens_f, axis=1)
    decay_cols = lax.dynamic_slice_in_dim(decay_weight, head * KEY_CHANNELS, KEY_CHANNELS, 1)
    bias_cols = lax.dynamic_slice_in_dim(decay_preact_bias, head * KEY_CHANNELS, KEY_CHANNELS)
    pre = jnp.einsum("srp,rc->spc", past_lowrank_cache, decay_cols, preferred_element_type=F32)
    gates = log_gate(pre + bias_cols) + jnp.transpose(head_extra_decay, (0, 2, 1))
    ids = place * positions + lax.broadcasted_iota(jnp.int32, (sequences, positions), 1)
    live = (ids < lengths[:, None])[:, :, None]
    gates = jnp.where(live, gates, 0.0)
    totals = jnp.sum(gates, axis=1)
    sq_high, sq_low = split_two(squares)
    low_row = jnp.concatenate(
        [
            product(scaled, low_rows).reshape(MEMBERS, 96),
            sq_high.reshape(MEMBERS, OWN),
            sq_low.reshape(MEMBERS, OWN),
            jnp.zeros((MEMBERS, 20), F32),
        ],
        axis=1,
    )[:, None, :]
    shared = jnp.concatenate(
        [
            product(scaled, query_weight).reshape(MEMBERS, OWN, KEY_CHANNELS),
            totals.reshape(MEMBERS, OWN, KEY_CHANNELS),
            low_row,
        ],
        axis=1,
    )
    owned = by_owner(
        jnp.concatenate(
            [
                product(scaled, key_weight)[:, None, :],
                product(scaled, value_weight).reshape(sequences, 2, 128),
                product(scaled, output_gate_weight).reshape(sequences, 2, 128),
            ],
            axis=1,
        )
    )
    first = jnp.concatenate(
        [copies(shared, GROUPS).reshape(32, 13, 128), owned], axis=1
    ).astype(BF)
    got = exchange(first.reshape(32, 9, 2, 128), KV).reshape(32, 18, 128).astype(F32)
    order = lax.broadcasted_iota(jnp.int32, (positions, positions), 0)
    later_ones = (lax.broadcasted_iota(jnp.int32, (positions, positions), 1) > order).astype(BF)
    high = gates.astype(BF)
    low = (gates - high.astype(F32)).astype(BF)
    suffix = jnp.einsum("ij,sjc->sic", later_ones, high, preferred_element_type=F32) + jnp.einsum(
        "ij,sjc->sic", later_ones, low, preferred_element_type=F32
    )
    weighted = jnp.where(live, past_key_cache.astype(F32) * jnp.exp(suffix), 0.0).astype(BF)
    state = jnp.einsum(
        "spc,spv->scv", weighted, past_value_cache, preferred_element_type=F32
    ).astype(BF)
    sums = jnp.sum(got, axis=0)
    later_totals = got[:, OWN : 2 * OWN]
    inv = lax.rsqrt((sums[12, 96:102] + sums[12, 102:108]) / D + NORM_EPSILON)[:, None]
    query = (inv * sums[:OWN]).astype(BF).astype(F32) * KEY_CHANNELS ** (-0.5)
    lowrank = (inv * sums[12, :96].reshape(OWN, 16)).astype(BF)
    fresh = log_gate(product(lowrank, decay_cols) + bias_cols)
    ends = group * MEMBERS + jnp.arange(MEMBERS)
    after = (jnp.arange(32)[None, :] > ends[:, None]).astype(F32)
    later = jnp.sum(after[:, :, None, None] * later_totals[None], axis=1)
    ready = query * jnp.exp(fresh + later)
    ready = jnp.concatenate([ready, jnp.zeros((MEMBERS, 2, 128), F32)], axis=1)
    mine = (jnp.arange(OWN) == group).astype(F32)[:, None]
    own_inv = jnp.sum(mine * inv)
    key_new = (own_inv * sums[13]).astype(BF).astype(F32)
    value_new = (own_inv * sums[14:16].reshape(DV)).astype(BF).astype(F32)
    outgate = (own_inv * sums[16:18].reshape(DV)).astype(BF)
    own_value = jnp.sum(jnp.sum(mine * query, axis=0) * key_new) * value_new
    whole = exchange(ready, "kvl")[:, :OWN].reshape(sequences, KEY_CHANNELS)
    part = jnp.einsum("sc,scv->sv", whole, state.astype(F32))
    at_own = (jnp.arange(sequences) == member * OWN + group) & (group < OWN)
    part = part + jnp.where(at_own[:, None], own_value[None, :], 0.0)
    second = jnp.concatenate(
        [
            part.reshape(MEMBERS, OWN, DV).astype(BF),
            jnp.broadcast_to(outgate, (MEMBERS, 2, DV)),
        ],
        axis=1,
    )
    second = copies(second, GROUPS).reshape(32, 8, DV)
    back = exchange(second, KV)
    mixed = jnp.sum(back[:, :OWN].astype(F32), axis=0)
    outgates = lax.dynamic_index_in_dim(
        back.reshape(GROUPS, MEMBERS, 8, DV)[:OWN, :, OWN], member, 1, keepdims=False
    ).astype(F32)
    mean_sq = jnp.mean(mixed * mixed, axis=1, keepdims=True)
    gated = (
        mixed * lax.rsqrt(mean_sq + NORM_EPSILON) * head_norm_gain * jax.nn.silu(outgates)
    ).astype(BF)
    columns = exchange(copies(output_weight, MEMBERS), "kvl")
    rows = jnp.einsum("sv,rvc->rsc", gated, columns, preferred_element_type=F32).astype(BF)
    rows = jnp.concatenate([rows, jnp.zeros((MEMBERS, 2, 128), BF)], axis=1)
    rows = jnp.broadcast_to(rows[:, None], (MEMBERS, 16, 8, 128)).reshape(64, 8, 128)
    rows = exchange(rows, ("kvl", *TP)).reshape(MEMBERS, 16, 8, 128)
    attention = jnp.sum(rows[:, :, :OWN].astype(F32), axis=1).reshape(sequences, width)
    residual = tokens_f + attention
    gain_two = lax.dynamic_slice_in_dim(feedforward_norm_gain, row_start, width)
    scaled_two = (residual * gain_two).astype(BF)
    square_parts = jnp.stack(split_two(jnp.sum(residual * residual, axis=1)), axis=1)
    wide = jnp.stack(
        [
            product(scaled_two, feedforward_gate_weight),
            product(scaled_two, feedforward_up_weight),
        ],
        axis=1,
    )
    units = wide.shape[2]
    third = jnp.concatenate(
        [wide, jnp.broadcast_to(square_parts[:, :, None], (sequences, 2, 128))], axis=2
    )
    third = exchange(by_owner(third).astype(BF), KV)
    sums_two = jnp.sum(third.astype(F32), axis=0)
    inv_two = lax.rsqrt((sums_two[0, units] + sums_two[1, units]) / D + NORM_EPSILON)
    hidden = (
        jax.nn.silu(inv_two * sums_two[0, :units]) * (inv_two * sums_two[1, :units])
    ).astype(BF)
    hidden = jnp.concatenate([hidden, jnp.zeros((1024 - units,), BF)]).reshape(8, 128)
    hidden = exchange(copies(hidden, 32), KV).reshape(GROUPS, MEMBERS, 1024)[:OWN, :, :units]
    hidden = jnp.swapaxes(hidden, 0, 1).reshape(sequences, units)
    down = product(hidden, feedforward_down_weight).astype(BF)
    down = exchange(copies(down, 16), TP)
    return (residual + jnp.sum(down.astype(F32), axis=0)).astype(BF)


def solution(mesh):
    finer = Mesh(mesh.devices.reshape(GROUPS, MEMBERS, 4, 4), (*KV, *TP))
    placed = (
        P(None, KV),
        P(),
        P(KV, TP),
        P(KV, TP),
        P(KV, TP),
        P(KV, TP),
        P(),
        P(),
        P(),
        P(),
        P(TP, KV),
        P(),
        P(KV, TP),
        P(KV, TP),
        P(TP, KV),
        P(None, KV, TP),
        P(None, KV, TP),
        P(None, None, KV),
        P(None, TP, KV),
        P(),
    )
    return jax.shard_map(
        shards, mesh=finer, in_specs=placed, out_specs=P(None, KV), check_vma=False
    )
```

```python
import jax
import jax.numpy as jnp
from jax import lax
from jax.experimental import pallas as pl
from jax.experimental.pallas import tpu as pltpu
from jax.sharding import Mesh
from jax.sharding import PartitionSpec as P

D = 4096
KEY_CHANNELS = 128
DV = 256
GROUPS = 8
MEMBERS = 4
OWN = 6
KV = ("kvh", "kvl")
TP = ("tp_0", "tp_1")
NORM_EPSILON = 1e-06
BF = jnp.bfloat16
F32 = jnp.float32


VMEM_LIMIT = 16 * 1024 * 1024


def exchange(array, axes):
    return lax.all_to_all(array, axes, split_axis=0, concat_axis=0, tiled=True)


def copies(array, size):
    return jnp.broadcast_to(array, (size, *array.shape))


def iota(shape, dim):
    return lax.broadcasted_iota(jnp.int32, shape, dim)


def dot(lhs, rhs, contract=((1,), (0,))):
    return lax.dot_general(lhs, rhs, (contract, ((), ())), preferred_element_type=F32)


def rounded(array):
    return array.astype(BF).astype(F32)


def log_gate(values):
    return (jnp.minimum(values, 0.0) - jnp.log(1.0 + jnp.exp(-jnp.abs(values)))) * 0.0625


def silu(values):
    return values / (1.0 + jnp.exp(-values))


def place_of():
    group, member = lax.axis_index("kvh"), lax.axis_index("kvl")
    return group, member, group * MEMBERS + member


def kernel_call(kernel, outs, scratch=(), hbm=(), flops=1_000_000, count=0, name=None):
    specs = [
        pl.BlockSpec(memory_space=pltpu.HBM if i in hbm else pltpu.VMEM) for i in range(count)
    ]
    many = isinstance(outs, (tuple, list))
    call = pl.pallas_call(
        kernel,
        out_shape=outs,
        in_specs=specs,
        out_specs=[pl.BlockSpec(memory_space=pltpu.VMEM)] * len(outs)
        if many
        else pl.BlockSpec(memory_space=pltpu.VMEM),
        scratch_shapes=list(scratch),
        cost_estimate=pl.CostEstimate(flops=flops, bytes_accessed=1_000_000, transcendentals=0),
        compiler_params=pltpu.CompilerParams(vmem_limit_bytes=VMEM_LIMIT),
        name=name,
    )
    return lambda *args: call(
        *(
            pltpu.with_memory_space_constraint(a, pltpu.HBM) if i in hbm else a
            for i, a in enumerate(args)
        )
    )


def fetched(pairs, sems):
    moves = [pltpu.make_async_copy(src, dst, sems.at[i]) for i, (src, dst) in enumerate(pairs)]
    for move in moves:
        move.start()
    return moves


def spread_rows(decay_cols):
    stacked = jnp.concatenate([decay_cols] * 8, axis=0)
    owner = lax.shift_right_logical(iota((128, 128), 0), 4)
    blocks = [jnp.where(owner == m, stacked, 0.0) for m in range(8)]
    seq_row = iota((16, 128), 0) & 7
    ones = [(seq_row == m).astype(F32) for m in range(8)]
    return jnp.concatenate(blocks, axis=1).astype(BF), jnp.concatenate(ones, axis=1).astype(BF)


def gate_inputs(b, lowcache, extra, blocks, ones, pre, add):
    pre[...] = dot(lowcache[128 * b : 128 * b + 128, :], blocks, ((0,), (0,)))
    lines = jnp.concatenate([extra[8 * b + m] for m in range(8)], axis=0)
    high = rounded(lines)
    both = jnp.concatenate([high, lines - high], axis=0).astype(BF)
    add[...] = dot(both, ones, ((0,), (0,)))


def start_kernel(
    lengths_h,
    lowcache_h,
    decay_h,
    bias_h,
    extra_h,
    tokens_h,
    gain_h,
    low_h,
    query_h,
    key_h,
    value_h,
    outgate_h,
    send,
    lengths,
    lowcache,
    decay,
    bias,
    extra,
    tokens,
    gain,
    low_w,
    query_w,
    key_w,
    value_w,
    outgate_w,
    pre,
    add,
    rows,
    sems,
):
    group, member, place = place_of()
    head = lax.axis_index(TP)
    head_lanes = pl.ds(pl.multiple_of(head * 128, 128), 128)
    place_lanes = pl.ds(pl.multiple_of(place * 128, 128), 128)
    moves = fetched(
        [
            (decay_h.at[:, head_lanes], decay),
            (lowcache_h, lowcache),
            (extra_h, extra),
            (bias_h, bias),
            (lengths_h, lengths),
            (tokens_h, tokens),
            (gain_h, gain),
            (low_h.at[:, place_lanes], low_w),
            (query_h, query_w),
            (key_h, key_w),
            (value_h, value_w),
            (outgate_h, outgate_w),
        ],
        sems,
    )
    ids = place * 192 + iota((192, 128), 0)
    for move in moves[:5]:
        move.wait()
    blocks, ones = spread_rows(decay[...].astype(F32))
    bias_row = bias[pl.ds(head, 1), :]
    for b in range(3):
        gate_inputs(b, lowcache, extra, blocks, ones, pre, add)
        for m in range(8):
            s, lanes = 8 * b + m, slice(128 * m, 128 * m + 128)
            gate = log_gate(pre[:, lanes] + bias_row) + add[:, lanes]
            gate = jnp.where(ids < lengths[s], gate, 0.0)
            rows[1, s : s + 1, :] = jnp.sum(gate, axis=0, keepdims=True)
    for move in moves[5:]:
        move.wait()
    tokens_f = tokens[...].astype(F32)
    scaled = (tokens_f * gain[pl.ds(place, 1), :]).astype(BF)
    rows[0] = dot(scaled, query_w[...])
    rows[2] = dot(scaled, key_w[...])
    value = dot(scaled, value_w[...])
    outgate = dot(scaled, outgate_w[...])
    low_t = low_w[...].astype(F32)
    low_t = jnp.concatenate([low_t] * OWN + [jnp.zeros((32, 128), F32)], axis=0).astype(BF)
    low = dot(scaled, low_t, ((1,), (1,)))
    squares = jnp.sum(tokens_f * tokens_f, axis=1, keepdims=True)
    high = rounded(squares)
    lane, row = iota((24, 128), 1), iota((24, 128), 0)
    owner = sum((row >= OWN * r).astype(jnp.int32) for r in range(1, MEMBERS))
    slot = row - OWN * owner
    line = jnp.where(lax.shift_right_logical(lane, 4) == slot, low, 0.0)
    line = jnp.where(lane >= 96, 0.0, line)
    line = jnp.where(lane == 96 + slot, high, line)
    line = jnp.where(lane == 102 + slot, squares - high, line)
    pick_row, pick_col = iota((8, 24), 0), iota((8, 24), 1)
    pick = ((pick_col >= OWN * pick_row) & (pick_col < OWN * pick_row + OWN)).astype(F32)
    line = dot(pick.astype(BF), line.astype(BF))
    for r in range(MEMBERS):
        for a in range(3):
            at = slice(OWN * r + 2 * a, OWN * r + 2 * a + 2)
            query_pair = rows[0, at, :].astype(BF)
            total_pair = rows[1, at, :].astype(BF)
            for g in range(GROUPS):
                send[MEMBERS * g + r, a] = query_pair
                send[MEMBERS * g + r, 3 + a] = total_pair
        for g in range(GROUPS):
            s, j = OWN * r + min(g, OWN - 1), MEMBERS * g + r
            one = jnp.concatenate([line[r : r + 1], rows[2, s : s + 1, :]], axis=0)
            send[j, 6] = one.astype(BF)
            send[j, 7] = halves(value[s : s + 1])
            send[j, 8] = halves(outgate[s : s + 1])


def halves(row):
    return jnp.concatenate([row[:, :128], row[:, 128:]], axis=0).astype(BF)


def state_kernel(
    lengths_h,
    lowcache_h,
    decay_h,
    bias_h,
    extra_h,
    keys_h,
    values_h,
    state,
    lengths,
    lowcache,
    decay,
    bias,
    extra,
    keys,
    values,
    pre,
    add,
    high,
    low,
    sems,
):
    _, _, place = place_of()
    head = lax.axis_index(TP)
    head_lanes = pl.ds(pl.multiple_of(head * 128, 128), 128)
    moves = fetched(
        [
            (decay_h.at[:, head_lanes], decay),
            (lowcache_h, lowcache),
            (extra_h, extra),
            (bias_h, bias),
            (lengths_h, lengths),
        ]
        + [
            (whole.at[8 * b : 8 * b + 8], part.at[8 * b : 8 * b + 8])
            for b in range(3)
            for whole, part in ((keys_h, keys), (values_h, values))
        ],
        sems,
    )
    later = (iota((192, 192), 1) > iota((192, 192), 0)).astype(F32).astype(BF)
    ids = place * 192 + iota((192, 128), 0)
    for move in moves[:5]:
        move.wait()
    blocks, ones = spread_rows(decay[...].astype(F32))
    bias_row = bias[pl.ds(head, 1), :]
    for b in range(3):
        gate_inputs(b, lowcache, extra, blocks, ones, pre, add)
        for m in range(8):
            lanes = slice(128 * m, 128 * m + 128)
            gate = log_gate(pre[:, lanes] + bias_row) + add[:, lanes]
            gate = jnp.where(ids < lengths[8 * b + m], gate, 0.0)
            top = gate.astype(BF)
            high[:, lanes] = top
            low[:, lanes] = (gate - top.astype(F32)).astype(BF)
        pre[...] = dot(later, high[...]) + dot(later, low[...])
        for move in moves[5 + 2 * b : 7 + 2 * b]:
            move.wait()
        for m in range(8):
            s, lanes = 8 * b + m, slice(128 * m, 128 * m + 128)
            weighted = keys[s].astype(F32) * jnp.exp(pre[:, lanes])
            weighted = jnp.where(ids < lengths[s], weighted, 0.0).astype(BF)
            state[128 * s : 128 * s + 128, :] = dot(weighted, values[s], ((0,), (0,))).astype(BF)


def query_kernel(got, decay_w, bias, ready, own_value, outgate, low_stack, held):
    group, member, place = place_of()
    head = lax.axis_index(TP)
    decay_cols = decay_w[:, pl.ds(pl.multiple_of(head * 128, 128), 128)].astype(F32)
    bias_row = bias[pl.ds(head, 1), :]
    stack = jnp.concatenate([decay_cols] * OWN + [jnp.zeros((32, 128), F32)], axis=0).astype(BF)

    def summed(a):
        return jnp.sum(got[:, a].astype(F32), axis=0)

    held[...] = jnp.zeros_like(held)
    for a in range(3):
        at = slice(2 * a, 2 * a + 2)
        held[MEMBERS, at, :] = summed(a)
        parts = [got[j, 3 + a].astype(F32) for j in range(32)]
        beyond = jnp.zeros((2, 128), F32)
        own = [jnp.zeros((2, 128), F32)] * MEMBERS
        for k in range(GROUPS):
            four = parts[MEMBERS * k : MEMBERS * k + MEMBERS]
            beyond = beyond + jnp.where(k > group, (four[0] + four[1]) + (four[2] + four[3]), 0.0)
            own = [o + jnp.where(k == group, f, 0.0) for o, f in zip(own, four)]
        for r in reversed(range(MEMBERS)):
            held[r, at, :] = beyond
            beyond = beyond + own[r]
    mixed_pair = summed(6)
    line, key_sum = mixed_pair[0:1], mixed_pair[1:2]
    lane, row = iota((8, 128), 1), iota((8, 128), 0)
    wide = jnp.broadcast_to(line, (8, 128))
    square = jnp.sum(
        jnp.where((row < OWN) & ((lane == 96 + row) | (lane == 102 + row)), wide, 0.0),
        axis=1,
        keepdims=True,
    )
    inv = lax.rsqrt(square * (1.0 / D) + NORM_EPSILON)
    low = jnp.where((lax.shift_right_logical(lane, 4) == row) & (row < OWN), wide, 0.0)
    fresh = log_gate(dot((inv * low).astype(BF), stack) + bias_row)
    query = rounded(inv * held[MEMBERS]) * KEY_CHANNELS ** (-0.5)
    for r in range(MEMBERS):
        ready[r] = query * jnp.exp(fresh + held[r])
    is_own = row == group
    own_query = jnp.sum(jnp.where(is_own, query, 0.0), axis=0, keepdims=True)
    own_inv = jnp.sum(jnp.where(is_own[:, :1], inv, 0.0), axis=0, keepdims=True)
    own = jnp.sum(own_query * rounded(own_inv * key_sum), axis=1, keepdims=True)
    pair = own * rounded(own_inv * summed(7))
    own_value[:, :128], own_value[:, 128:] = pair[0:1], pair[1:2]
    pair = rounded(own_inv * summed(8))
    outgate[:, :128], outgate[:, 128:] = pair[0:1], pair[1:2]


def heads_kernel(whole, state, own_value, outgate, send):
    group, member, place = place_of()
    query = whole[...].reshape(32, 128)
    high = rounded(query)
    both = jnp.concatenate([high, query - high], axis=0)
    row = iota((64, 128), 0) & 31
    spread = jnp.concatenate(
        [
            jnp.where(row == 8 * (s // OWN) + s % OWN, both, 0.0).astype(BF)
            for s in range(24)
        ],
        axis=1,
    )
    part = dot(spread, state[...])
    part = part[:32] + part[32:]
    row = iota((32, DV), 0)
    part = part + jnp.where(row == 8 * member + group, own_value[...], 0.0)
    gate_pair = halves(outgate[...])
    for r in range(MEMBERS):
        for k in range(OWN):
            pair = halves(part[8 * r + k : 8 * r + k + 1])
            for g in range(GROUPS):
                send[MEMBERS * g + r, k] = pair
        for g in range(GROUPS):
            send[MEMBERS * g + r, OWN] = gate_pair


def gating_kernel(back, own, from_one, from_two, from_three, gain, send, mixed_rows, gate_rows):
    group, member, place = place_of()
    mixed_rows[...] = jnp.zeros_like(mixed_rows)
    gate_rows[...] = jnp.zeros_like(gate_rows)
    for k in range(OWN):
        pair = jnp.sum(back[:, k].astype(F32), axis=0)
        mixed_rows[k : k + 1, :128], mixed_rows[k : k + 1, 128:] = pair[0:1], pair[1:2]
        pair = back[MEMBERS * k + member, OWN].astype(F32)
        gate_rows[k : k + 1, :128], gate_rows[k : k + 1, 128:] = pair[0:1], pair[1:2]
    mixed = mixed_rows[...]
    mean_sq = jnp.sum(mixed * mixed, axis=1, keepdims=True) * (1.0 / DV)
    gated = mixed * lax.rsqrt(mean_sq + NORM_EPSILON) * gain[...] * silu(gate_rows[...])
    gated = gated.astype(BF)
    for d, columns in enumerate((own, from_one, from_two, from_three)):
        rows = dot(gated, columns[...])
        source = (member + MEMBERS - d) & (MEMBERS - 1)
        for a in range(3):
            pair = rows[2 * a : 2 * a + 2].astype(BF)
            for h in range(16):
                send[16 * source + h, a] = pair


def wide_kernel(rows, tokens, gain, gate_w, up_w, send, residual, held):
    group, member, place = place_of()
    for r in range(MEMBERS):
        for a in range(3):
            part = jnp.sum(rows[16 * r : 16 * r + 16, a].astype(F32), axis=0)
            held[OWN * r + 2 * a : OWN * r + 2 * a + 2, :] = part
    total = held[...] + tokens[...].astype(F32)
    residual[...] = total
    scaled = (total * gain[pl.ds(place, 1), :]).astype(BF)
    square = jnp.sum(total * total, axis=1, keepdims=True)
    high = rounded(square)
    gate, up = dot(scaled, gate_w[...]), dot(scaled, up_w[...])
    gate = jnp.concatenate([gate, jnp.broadcast_to(high, (24, 128))], axis=1)
    up = jnp.concatenate([up, jnp.broadcast_to(square - high, (24, 128))], axis=1)
    for g in range(GROUPS):
        for r in range(MEMBERS):
            s = OWN * r + min(g, OWN - 1)
            pair = jnp.concatenate([gate[s : s + 1], up[s : s + 1]], axis=0)
            send[MEMBERS * g + r] = pair.astype(BF)


def hidden_kernel(got, send):
    pair = jnp.sum(got[...].astype(F32), axis=0)
    units = pair.shape[1] - 128
    square = pair[0:1, units : units + 1] + pair[1:2, units : units + 1]
    inv = lax.rsqrt(square * (1.0 / D) + NORM_EPSILON)
    hidden = silu(inv * pair[0:1, :units]) * (inv * pair[1:2, :units])
    wide = send.shape[2]
    rest = jnp.concatenate(
        [hidden[:, wide:], jnp.zeros((1, 2 * wide - units), F32)], axis=1
    )
    pair = jnp.concatenate([hidden[:, :wide], rest], axis=0).astype(BF)
    for j in range(32):
        send[j] = pair


def down_kernel(got, down_w, send, held):
    units, wide = down_w.shape[0], got.shape[2]
    for r in range(MEMBERS):
        for g in range(OWN):
            s = OWN * r + g
            pair = got[MEMBERS * g + r].astype(F32)
            held[s : s + 1, :wide] = pair[0:1]
            held[s : s + 1, wide:units] = pair[1:2, : units - wide]
    total = dot(held[...].astype(BF), down_w[...]).astype(BF)
    for h in range(16):
        send[h] = total


def shape(dtype, *dims):
    return jax.ShapeDtypeStruct(dims, dtype)


def shards(
    tokens,
    attention_norm_gain,
    query_weight,
    key_weight,
    value_weight,
    output_gate_weight,
    lowrank_weight,
    decay_weight,
    decay_preact_bias,
    head_norm_gain,
    output_weight,
    feedforward_norm_gain,
    feedforward_gate_weight,
    feedforward_up_weight,
    feedforward_down_weight,
    past_key_cache,
    past_value_cache,
    past_lowrank_cache,
    head_extra_decay,
    lengths,
):
    bias = decay_preact_bias.reshape(16, 128)
    lowcache = past_lowrank_cache.reshape(384, 192)
    gate_scratch = [
        pltpu.SMEM((24,), jnp.int32),
        pltpu.VMEM((384, 192), BF),
        pltpu.VMEM((16, 128), BF),
        pltpu.VMEM((16, 128), F32),
        pltpu.VMEM((24, 1, 192), F32),
    ]
    first = kernel_call(
        start_kernel,
        pltpu.VMEM((32, 9, 2, 128), BF),
        scratch=gate_scratch
        + [
            pltpu.VMEM((24, 128), BF),
            pltpu.VMEM((32, 128), F32),
            pltpu.VMEM((16, 128), BF),
            pltpu.VMEM((128, 128), BF),
            pltpu.VMEM((128, 128), BF),
            pltpu.VMEM((128, DV), BF),
            pltpu.VMEM((128, DV), BF),
            pltpu.VMEM((192, 1024), F32),
            pltpu.VMEM((192, 1024), F32),
            pltpu.VMEM((3, 24, 128), F32),
            pltpu.SemaphoreType.DMA((12,)),
        ],
        count=12,
        hbm=range(12),
        name="start",
    )(
        lengths,
        lowcache,
        decay_weight,
        bias,
        head_extra_decay,
        tokens,
        attention_norm_gain.reshape(32, 128),
        lowrank_weight.T,
        query_weight,
        key_weight,
        value_weight,
        output_gate_weight,
    )
    late_cache, first = lax.optimization_barrier((lowcache, first))
    got = exchange(first, KV)
    state = kernel_call(
        state_kernel,
        pltpu.VMEM((3072, DV), BF),
        scratch=gate_scratch
        + [
            pltpu.VMEM((24, 192, 128), BF),
            pltpu.VMEM((24, 192, DV), BF),
            pltpu.VMEM((192, 1024), F32),
            pltpu.VMEM((192, 1024), F32),
            pltpu.VMEM((192, 1024), BF),
            pltpu.VMEM((192, 1024), BF),
            pltpu.SemaphoreType.DMA((11,)),
        ],
        count=7,
        hbm=range(7),
        flops=20_000_000_000,
        name="state",
    )(
        lengths,
        late_cache,
        decay_weight,
        bias,
        head_extra_decay,
        past_key_cache,
        past_value_cache,
    )
    late, state = lax.optimization_barrier((output_weight, state))
    from_two = lax.ppermute(late, "kvl", [(m, m ^ 2) for m in range(MEMBERS)])
    got, state, from_two = lax.optimization_barrier((got, state, from_two))
    ready, own_value, outgate = kernel_call(
        query_kernel,
        (shape(F32, MEMBERS, 8, 128), shape(F32, 1, DV), shape(F32, 1, DV)),
        scratch=[pltpu.VMEM((8, 128), F32), pltpu.VMEM((MEMBERS + 1, 8, 128), F32)],
        count=3,
        name="query",
    )(got, decay_weight, bias)
    whole = exchange(ready, "kvl")
    second = kernel_call(heads_kernel, shape(BF, 32, 7, 2, 128), count=4, name="heads")(
        whole, state, own_value, outgate
    )
    late, second = lax.optimization_barrier((output_weight, second))
    back = exchange(second, KV)
    from_one, from_three = (
        lax.ppermute(late, "kvl", [(m, (m + d) % MEMBERS) for m in range(MEMBERS)])
        for d in (1, 3)
    )
    back, columns = lax.optimization_barrier((back, (output_weight, from_one, from_two, from_three)))
    rows = kernel_call(
        gating_kernel,
        shape(BF, 64, 3, 2, 128),
        scratch=[pltpu.VMEM((8, DV), F32), pltpu.VMEM((8, DV), F32)],
        count=6,
        name="gating",
    )(back, *columns, head_norm_gain.reshape(1, DV))
    rows = exchange(rows, ("kvl", *TP))
    units = feedforward_gate_weight.shape[1]
    third, residual = kernel_call(
        wide_kernel,
        (shape(BF, 32, 2, units + 128), shape(F32, 24, 128)),
        scratch=[pltpu.VMEM((24, 128), F32)],
        count=5,
        name="wide",
    )(
        rows,
        tokens,
        feedforward_norm_gain.reshape(32, 128),
        feedforward_gate_weight,
        feedforward_up_weight,
    )
    third = exchange(third, KV)
    hidden = kernel_call(
        hidden_kernel,
        shape(BF, 32, 2, 384),
        count=1,
        name="hidden",
    )(third)
    hidden = exchange(hidden, KV)
    down = kernel_call(
        down_kernel,
        shape(BF, 16, 24, 128),
        scratch=[pltpu.VMEM((24, units), F32)],
        count=2,
        name="down",
    )(hidden, feedforward_down_weight)
    down = exchange(down, TP)
    return (residual + jnp.sum(down.astype(F32), axis=0)).astype(BF)


def solution(mesh):
    finer = Mesh(mesh.devices.reshape(GROUPS, MEMBERS, 4, 4), (*KV, *TP))
    placed = (
        P(None, KV),
        P(),
        P(KV, TP),
        P(KV, TP),
        P(KV, TP),
        P(KV, TP),
        P(),
        P(),
        P(),
        P(),
        P(TP, KV),
        P(),
        P(KV, TP),
        P(KV, TP),
        P(TP, KV),
        P(None, KV, TP),
        P(None, KV, TP),
        P(None, None, KV),
        P(None, TP, KV),
        P(),
    )
    return jax.shard_map(
        shards, mesh=finer, in_specs=placed, out_specs=P(None, KV), check_vma=False
    )
```

```python
import jax
import jax.numpy as jnp
from jax import lax
from jax.experimental import pallas as pl
from jax.experimental.pallas import tpu as pltpu
from jax.sharding import Mesh
from jax.sharding import PartitionSpec as P

D = 4096
KEY_CHANNELS = 128
DV = 256
GROUPS = 8
MEMBERS = 4
OWN = 6
Z = ("za", "zb", "zc")
KVL = ("zc", "core")
NEAR = ("zb", "zc", "core")
KV = (*Z, "core")
TP = ("tp_0", "tp_1")
NORM_EPSILON = 1e-06
BF = jnp.bfloat16
F32 = jnp.float32


BIG = 1e9
VMEM_LIMIT = 16 * 1024 * 1024


def exchange(array, axes):
    return lax.all_to_all(array, axes, split_axis=0, concat_axis=0, tiled=True)


def copies(array, size):
    return jnp.broadcast_to(array, (size, *array.shape))


def iota(shape, dim):
    return lax.broadcasted_iota(jnp.int32, shape, dim)


def dot(lhs, rhs, contract=((1,), (0,))):
    return lax.dot_general(lhs, rhs, (contract, ((), ())), preferred_element_type=F32)


def rounded(array):
    return array.astype(BF).astype(F32)


def log_gate(values):
    return (jnp.minimum(values, 0.0) - jnp.log(1.0 + jnp.exp(-jnp.abs(values)))) * 0.0625


def silu(values):
    return values / (1.0 + jnp.exp(-values))


def place_of():
    group, member = lax.axis_index(("za", "zb")), lax.axis_index(KVL)
    return group, member, group * MEMBERS + member


def kernel_call(kernel, outs, scratch=(), hbm=(), flops=1_000_000, count=0, name=None):
    specs = [
        pl.BlockSpec(memory_space=pltpu.HBM if i in hbm else pltpu.VMEM) for i in range(count)
    ]
    many = isinstance(outs, (tuple, list))
    call = pl.pallas_call(
        kernel,
        out_shape=outs,
        in_specs=specs,
        out_specs=[pl.BlockSpec(memory_space=pltpu.VMEM)] * len(outs)
        if many
        else pl.BlockSpec(memory_space=pltpu.VMEM),
        scratch_shapes=list(scratch),
        cost_estimate=pl.CostEstimate(flops=flops, bytes_accessed=1_000_000, transcendentals=0),
        compiler_params=pltpu.CompilerParams(vmem_limit_bytes=VMEM_LIMIT),
        name=name,
    )
    return lambda *args: call(
        *(
            pltpu.with_memory_space_constraint(a, pltpu.HBM) if i in hbm else a
            for i, a in enumerate(args)
        )
    )


def fetched(pairs, sems):
    moves = [pltpu.make_async_copy(src, dst, sems.at[i]) for i, (src, dst) in enumerate(pairs)]
    for move in moves:
        move.start()
    return moves


def spread_rows(decay_cols):
    stacked = jnp.concatenate([decay_cols] * 8, axis=0)
    owner = lax.shift_right_logical(iota((128, 128), 0), 4)
    blocks = [jnp.where(owner == m, stacked, 0.0) for m in range(8)]
    seq_row = iota((16, 128), 0) & 7
    ones = [(seq_row == m).astype(F32) for m in range(8)]
    return jnp.concatenate(blocks, axis=1).astype(BF), jnp.concatenate(ones, axis=1).astype(BF)


def gate_inputs(b, lowcache, extra, blocks, ones, pre, add):
    pre[...] = dot(lowcache[128 * b : 128 * b + 128, :], blocks, ((0,), (0,)))
    lines = jnp.concatenate([extra[8 * b + m] for m in range(8)], axis=0)
    high = rounded(lines)
    both = jnp.concatenate([high, lines - high], axis=0).astype(BF)
    add[...] = dot(both, ones, ((0,), (0,)))


def start_kernel(
    lengths_h,
    lowcache_h,
    decay_h,
    bias_h,
    extra_h,
    tokens_h,
    gain_h,
    low_h,
    query_h,
    key_h,
    value_h,
    outgate_h,
    send,
    lengths,
    lowcache,
    decay,
    bias,
    extra,
    tokens,
    gain,
    low_w,
    query_w,
    key_w,
    value_w,
    outgate_w,
    pre,
    rows,
    sems,
):
    group, member, place = place_of()
    head = lax.axis_index(TP)
    head_lanes = pl.ds(pl.multiple_of(head * 128, 128), 128)
    place_lanes = pl.ds(pl.multiple_of(place * 128, 128), 128)
    moves = fetched(
        [
            (decay_h.at[:, head_lanes], decay),
            (lowcache_h, lowcache),
            (extra_h, extra),
            (bias_h, bias),
            (lengths_h, lengths),
            (tokens_h, tokens),
            (gain_h, gain),
            (low_h.at[:, place_lanes], low_w),
            (query_h, query_w),
            (key_h, key_w),
            (value_h, value_w),
            (outgate_h, outgate_w),
        ],
        sems,
    )
    start = place * 192
    ids = start + iota((192, 128), 0)
    for move in moves[:5]:
        move.wait()
    blocks = spread_rows(decay[...].astype(F32))[0]
    bias_row = bias[pl.ds(head, 1), :]
    line_ids = start + iota((1, 192), 1)
    for b in range(3):
        pre[...] = dot(lowcache[128 * b : 128 * b + 128, :], blocks, ((0,), (0,)))
        for m in range(8):
            s, lanes = 8 * b + m, slice(128 * m, 128 * m + 128)
            value = jnp.where(ids < lengths[s], pre[:, lanes] + bias_row, BIG)
            factor = (1.0 + jnp.exp(-jnp.abs(value))).reshape(24, 8, 128)
            while factor.shape[0] > 3:
                half = factor.shape[0] // 2
                factor = factor[:half] * factor[half:]
            factor = factor[0] * factor[1] * factor[2]
            below = jnp.sum(jnp.minimum(value, 0.0).reshape(24, 8, 128), axis=0)
            gate = jnp.sum(below - jnp.log(factor), axis=0, keepdims=True) * 0.0625
            line = jnp.where(line_ids < lengths[s], extra[s], 0.0)
            rows[1, s : s + 1, :] = gate + jnp.sum(line, axis=1, keepdims=True)
    for move in moves[5:]:
        move.wait()
    tokens_f = tokens[...].astype(F32)
    scaled = (tokens_f * gain[pl.ds(place, 1), :]).astype(BF)
    rows[0] = dot(scaled, query_w[...])
    rows[2] = dot(scaled, key_w[...])
    value = dot(scaled, value_w[...])
    outgate = dot(scaled, outgate_w[...])
    low_t = low_w[...].astype(F32)
    low_t = jnp.concatenate([low_t] * OWN + [jnp.zeros((32, 128), F32)], axis=0).astype(BF)
    low = dot(scaled, low_t, ((1,), (1,)))
    squares = jnp.sum(tokens_f * tokens_f, axis=1, keepdims=True)
    high = rounded(squares)
    lane, row = iota((24, 128), 1), iota((24, 128), 0)
    owner = sum((row >= OWN * r).astype(jnp.int32) for r in range(1, MEMBERS))
    slot = row - OWN * owner
    line = jnp.where(lax.shift_right_logical(lane, 4) == slot, low, 0.0)
    line = jnp.where(lane >= 96, 0.0, line)
    line = jnp.where(lane == 96 + slot, high, line)
    line = jnp.where(lane == 102 + slot, squares - high, line)
    pick_row, pick_col = iota((8, 24), 0), iota((8, 24), 1)
    pick = ((pick_col >= OWN * pick_row) & (pick_col < OWN * pick_row + OWN)).astype(F32)
    line = dot(pick.astype(BF), line.astype(BF))
    for r in range(MEMBERS):
        for a in range(3):
            at = slice(OWN * r + 2 * a, OWN * r + 2 * a + 2)
            query_pair = rows[0, at, :].astype(BF)
            total_pair = rows[1, at, :].astype(BF)
            for g in range(GROUPS):
                send[MEMBERS * g + r, a] = query_pair
                send[MEMBERS * g + r, 3 + a] = total_pair
        for g in range(GROUPS):
            s, j = OWN * r + min(g, OWN - 1), MEMBERS * g + r
            one = jnp.concatenate([line[r : r + 1], rows[2, s : s + 1, :]], axis=0)
            send[j, 6] = one.astype(BF)
            send[j, 7] = halves(value[s : s + 1])
            send[j, 8] = halves(outgate[s : s + 1])


def halves(row):
    return jnp.concatenate([row[:, :128], row[:, 128:]], axis=0).astype(BF)


def state_kernel(
    lengths_h,
    lowcache_h,
    decay_h,
    bias_h,
    extra_h,
    keys_h,
    values_h,
    state,
    lengths,
    lowcache,
    decay,
    bias,
    extra,
    keys,
    values,
    pre,
    add,
    high,
    low,
    sems,
):
    _, _, place = place_of()
    head = lax.axis_index(TP)
    head_lanes = pl.ds(pl.multiple_of(head * 128, 128), 128)
    moves = fetched(
        [
            (decay_h.at[:, head_lanes], decay),
            (lowcache_h, lowcache),
            (extra_h, extra),
            (bias_h, bias),
            (lengths_h, lengths),
        ]
        + [
            (whole.at[8 * b : 8 * b + 8], part.at[8 * b : 8 * b + 8])
            for b in range(3)
            for whole, part in ((keys_h, keys), (values_h, values))
        ],
        sems,
    )
    later = (iota((192, 192), 1) > iota((192, 192), 0)).astype(F32).astype(BF)
    ids = place * 192 + iota((192, 128), 0)
    for move in moves[:5]:
        move.wait()
    blocks, ones = spread_rows(decay[...].astype(F32))
    bias_row = bias[pl.ds(head, 1), :]
    for b in range(3):
        gate_inputs(b, lowcache, extra, blocks, ones, pre, add)
        for m in range(8):
            lanes = slice(128 * m, 128 * m + 128)
            gate = log_gate(pre[:, lanes] + bias_row) + add[:, lanes]
            gate = jnp.where(ids < lengths[8 * b + m], gate, 0.0)
            top = gate.astype(BF)
            high[:, lanes] = top
            low[:, lanes] = (gate - top.astype(F32)).astype(BF)
        pre[...] = dot(later, high[...]) + dot(later, low[...])
        for move in moves[5 + 2 * b : 7 + 2 * b]:
            move.wait()
        for m in range(8):
            s, lanes = 8 * b + m, slice(128 * m, 128 * m + 128)
            weighted = keys[s].astype(F32) * jnp.exp(pre[:, lanes])
            weighted = jnp.where(ids < lengths[s], weighted, 0.0).astype(BF)
            state[128 * s : 128 * s + 128, :] = dot(weighted, values[s], ((0,), (0,))).astype(BF)


def query_kernel(got, decay_w, bias, ready, own_value, outgate, low_stack, held):
    group, member, place = place_of()
    head = lax.axis_index(TP)
    decay_cols = decay_w[:, pl.ds(pl.multiple_of(head * 128, 128), 128)].astype(F32)
    bias_row = bias[pl.ds(head, 1), :]
    stack = jnp.concatenate([decay_cols] * OWN + [jnp.zeros((32, 128), F32)], axis=0).astype(BF)

    def summed(a):
        return jnp.sum(got[:, a].astype(F32), axis=0)

    held[...] = jnp.zeros_like(held)
    for a in range(3):
        at = slice(2 * a, 2 * a + 2)
        held[MEMBERS, at, :] = summed(a)
        parts = [got[j, 3 + a].astype(F32) for j in range(32)]
        beyond = jnp.zeros((2, 128), F32)
        own = [jnp.zeros((2, 128), F32)] * MEMBERS
        for k in range(GROUPS):
            four = parts[MEMBERS * k : MEMBERS * k + MEMBERS]
            beyond = beyond + jnp.where(k > group, (four[0] + four[1]) + (four[2] + four[3]), 0.0)
            own = [o + jnp.where(k == group, f, 0.0) for o, f in zip(own, four)]
        for r in reversed(range(MEMBERS)):
            held[r, at, :] = beyond
            beyond = beyond + own[r]
    mixed_pair = summed(6)
    line, key_sum = mixed_pair[0:1], mixed_pair[1:2]
    lane, row = iota((8, 128), 1), iota((8, 128), 0)
    wide = jnp.broadcast_to(line, (8, 128))
    square = jnp.sum(
        jnp.where((row < OWN) & ((lane == 96 + row) | (lane == 102 + row)), wide, 0.0),
        axis=1,
        keepdims=True,
    )
    inv = lax.rsqrt(square * (1.0 / D) + NORM_EPSILON)
    low = jnp.where((lax.shift_right_logical(lane, 4) == row) & (row < OWN), wide, 0.0)
    fresh = log_gate(dot((inv * low).astype(BF), stack) + bias_row)
    query = rounded(inv * held[MEMBERS]) * KEY_CHANNELS ** (-0.5)
    for r in range(MEMBERS):
        ready[r] = query * jnp.exp(fresh + held[r])
    is_own = row == group
    own_query = jnp.sum(jnp.where(is_own, query, 0.0), axis=0, keepdims=True)
    own_inv = jnp.sum(jnp.where(is_own[:, :1], inv, 0.0), axis=0, keepdims=True)
    own = jnp.sum(own_query * rounded(own_inv * key_sum), axis=1, keepdims=True)
    pair = own * rounded(own_inv * summed(7))
    own_value[:, :128], own_value[:, 128:] = pair[0:1], pair[1:2]
    pair = rounded(own_inv * summed(8))
    outgate[:, :128], outgate[:, 128:] = pair[0:1], pair[1:2]


def heads_kernel(whole, state, own_value, outgate, send):
    group, member, place = place_of()
    query = whole[...].reshape(32, 128)
    high = rounded(query)
    both = jnp.concatenate([high, query - high], axis=0)
    row = iota((64, 128), 0) & 31
    spread = jnp.concatenate(
        [
            jnp.where(row == 8 * (s // OWN) + s % OWN, both, 0.0).astype(BF)
            for s in range(24)
        ],
        axis=1,
    )
    part = dot(spread, state[...])
    part = part[:32] + part[32:]
    row = iota((32, DV), 0)
    part = part + jnp.where(row == 8 * member + group, own_value[...], 0.0)
    gate_pair = halves(outgate[...])
    for r in range(MEMBERS):
        for k in range(OWN):
            pair = halves(part[8 * r + k : 8 * r + k + 1])
            for g in range(GROUPS):
                send[MEMBERS * g + r, k] = pair
        for g in range(GROUPS):
            send[MEMBERS * g + r, OWN] = gate_pair


def gating_kernel(back, gain, send, mixed_rows, gate_rows):
    group, member, place = place_of()
    mixed_rows[...] = jnp.zeros_like(mixed_rows)
    gate_rows[...] = jnp.zeros_like(gate_rows)
    for k in range(OWN):
        pair = jnp.sum(back[:, k].astype(F32), axis=0)
        mixed_rows[k : k + 1, :128], mixed_rows[k : k + 1, 128:] = pair[0:1], pair[1:2]
        pair = back[MEMBERS * k + member, OWN].astype(F32)
        gate_rows[k : k + 1, :128], gate_rows[k : k + 1, 128:] = pair[0:1], pair[1:2]
    mixed = mixed_rows[...]
    mean_sq = jnp.sum(mixed * mixed, axis=1, keepdims=True) * (1.0 / DV)
    gated = mixed * lax.rsqrt(mean_sq + NORM_EPSILON) * gain[...] * silu(gate_rows[...])
    gated = gated.astype(BF)
    for r in range(MEMBERS):
        send[r] = gated


def output_kernel(gated, output_w, send, held):
    rows = dot(gated[...].reshape(32, DV), output_w[...])
    for r in range(MEMBERS):
        held[OWN * r : OWN * r + OWN, :] = rows[8 * r : 8 * r + OWN]
    rows = held[...].astype(BF)
    for h in range(32):
        send[h] = rows


def pack_kernel(gate_w, up_w, tokens, send):
    units = gate_w.shape[1]
    half = units // 2
    for i, weights in enumerate((gate_w, up_w)):
        whole = weights[...].astype(F32)
        for c in range(2):
            part = whole[:, half * c : half * c + half]
            zeros = jnp.zeros((128, send.shape[3] - half), F32)
            send[c, i, :128, :] = jnp.concatenate([part, zeros], axis=1).astype(BF)
            send[c, i, 128:, :128] = tokens[...]


def wide_kernel(rows, gain, halves_w, send, residual):
    core = lax.axis_index("core")
    _, _, place = place_of()
    gate = up = square = 0.0
    for c in range(2):
        total = jnp.sum(rows[16 * c : 16 * c + 16].astype(F32), axis=0)
        total = total + halves_w[c, core, 0, 128:, :128].astype(F32)

        @pl.when(core == c)
        def _():
            residual[...] = total

        scaled = (total * gain[pl.ds(place - core + c, 1), :]).astype(BF)
        square += jnp.sum(total * total, axis=1, keepdims=True)
        gate += dot(scaled, halves_w[c, core, 0, :128, :])
        up += dot(scaled, halves_w[c, core, 1, :128, :])
    high = rounded(square)
    spare = iota(gate.shape, 1) == gate.shape[1] - 1
    gate = jnp.where(spare, high, gate)
    up = jnp.where(spare, square - high, up)
    for s in range(24):
        pair = jnp.concatenate([gate[s : s + 1], up[s : s + 1]], axis=0).astype(BF)
        for z in range(4):
            send[4 * z + s // OWN, s % OWN] = pair


def hidden_kernel(got, send, gates, ups):
    wide = send.shape[2]
    gates[...] = jnp.zeros_like(gates)
    ups[...] = jnp.zeros_like(ups)
    for k in range(OWN):
        pair = jnp.sum(got[:, k].astype(F32), axis=0)
        gates[k : k + 1, :] = pair[0:1]
        ups[k : k + 1, :] = pair[1:2]
    gate, up = gates[...], ups[...]
    square = gate[:, wide - 1 :] + up[:, wide - 1 :]
    inv = lax.rsqrt(square * (1.0 / D) + NORM_EPSILON)
    hidden = (silu(inv * gate) * (inv * up)).astype(BF)
    for j in range(8):
        send[j] = hidden


def down_kernel(got, down_w, send, held):
    half = down_w.shape[0] // 2
    total = 0.0
    for c in range(2):
        for z in range(4):
            held[OWN * z : OWN * z + OWN, :] = got[2 * z + c].astype(F32)[:OWN]
        total += dot(held[...].astype(BF)[:, :half], down_w[half * c : half * c + half, :])
    total = total.astype(BF)
    for h in range(16):
        send[h] = total


def shape(dtype, *dims):
    return jax.ShapeDtypeStruct(dims, dtype)


def shards(
    tokens,
    attention_norm_gain,
    query_weight,
    key_weight,
    value_weight,
    output_gate_weight,
    lowrank_weight,
    decay_weight,
    decay_preact_bias,
    head_norm_gain,
    output_weight,
    feedforward_norm_gain,
    feedforward_gate_weight,
    feedforward_up_weight,
    feedforward_down_weight,
    past_key_cache,
    past_value_cache,
    past_lowrank_cache,
    head_extra_decay,
    lengths,
):
    bias = decay_preact_bias.reshape(16, 128)
    lowcache = past_lowrank_cache.reshape(384, 192)
    gate_scratch = [
        pltpu.SMEM((24,), jnp.int32),
        pltpu.VMEM((384, 192), BF),
        pltpu.VMEM((16, 128), BF),
        pltpu.VMEM((16, 128), F32),
        pltpu.VMEM((24, 1, 192), F32),
    ]
    first = kernel_call(
        start_kernel,
        pltpu.VMEM((32, 9, 2, 128), BF),
        scratch=gate_scratch
        + [
            pltpu.VMEM((24, 128), BF),
            pltpu.VMEM((32, 128), F32),
            pltpu.VMEM((16, 128), BF),
            pltpu.VMEM((128, 128), BF),
            pltpu.VMEM((128, 128), BF),
            pltpu.VMEM((128, DV), BF),
            pltpu.VMEM((128, DV), BF),
            pltpu.VMEM((192, 1024), F32),
            pltpu.VMEM((3, 24, 128), F32),
            pltpu.SemaphoreType.DMA((12,)),
        ],
        count=12,
        hbm=range(12),
        name="start",
    )(
        lengths,
        lowcache,
        decay_weight,
        bias,
        head_extra_decay,
        tokens,
        attention_norm_gain.reshape(32, 128),
        lowrank_weight.T,
        query_weight,
        key_weight,
        value_weight,
        output_gate_weight,
    )
    late_cache, first = lax.optimization_barrier((lowcache, first))
    got = exchange(first, KV)
    state = kernel_call(
        state_kernel,
        pltpu.VMEM((3072, DV), BF),
        scratch=gate_scratch
        + [
            pltpu.VMEM((24, 192, 128), BF),
            pltpu.VMEM((24, 192, DV), BF),
            pltpu.VMEM((192, 1024), F32),
            pltpu.VMEM((192, 1024), F32),
            pltpu.VMEM((192, 1024), BF),
            pltpu.VMEM((192, 1024), BF),
            pltpu.SemaphoreType.DMA((11,)),
        ],
        count=7,
        hbm=range(7),
        flops=20_000_000_000,
        name="state",
    )(
        lengths,
        late_cache,
        decay_weight,
        bias,
        head_extra_decay,
        past_key_cache,
        past_value_cache,
    )
    gate_w, up_w, state = lax.optimization_barrier(
        (feedforward_gate_weight, feedforward_up_weight, state)
    )
    units = feedforward_gate_weight.shape[1]
    wide = -(-(units // 2 + 1) // 128) * 128
    halves_w = kernel_call(
        pack_kernel,
        shape(BF, 2, 2, 152, wide),
        count=3,
        name="pack",
    )(gate_w, up_w, tokens)
    halves_w = lax.all_gather(halves_w, "core")
    got, state, halves_w = lax.optimization_barrier((got, state, halves_w))
    ready, own_value, outgate = kernel_call(
        query_kernel,
        (shape(F32, MEMBERS, 8, 128), shape(F32, 1, DV), shape(F32, 1, DV)),
        scratch=[pltpu.VMEM((8, 128), F32), pltpu.VMEM((MEMBERS + 1, 8, 128), F32)],
        count=3,
        name="query",
    )(got, decay_weight, bias)
    whole = exchange(ready, KVL)
    second = kernel_call(heads_kernel, shape(BF, 32, 7, 2, 128), count=4, name="heads")(
        whole, state, own_value, outgate
    )
    back = exchange(second, KV)
    gated = kernel_call(
        gating_kernel,
        shape(BF, MEMBERS, 8, DV),
        scratch=[pltpu.VMEM((8, DV), F32), pltpu.VMEM((8, DV), F32)],
        count=2,
        name="gating",
    )(back, head_norm_gain.reshape(1, DV))
    gated = exchange(gated, KVL)
    rows = kernel_call(
        output_kernel,
        shape(BF, 32, 24, 128),
        scratch=[pltpu.VMEM((24, 128), F32)],
        count=2,
        name="output",
    )(gated, output_weight)
    rows = exchange(rows, ("core", *TP))
    third, residual = kernel_call(
        wide_kernel,
        (shape(BF, 16, OWN, 2, wide), shape(F32, 24, 128)),
        count=3,
        name="wide",
    )(rows, feedforward_norm_gain.reshape(32, 128), halves_w)
    third = exchange(third, Z)
    hidden = kernel_call(
        hidden_kernel,
        shape(BF, 8, 8, wide),
        scratch=[pltpu.VMEM((8, wide), F32)] * 2,
        count=1,
        name="hidden",
    )(third)
    hidden = exchange(hidden, NEAR)
    down = kernel_call(
        down_kernel,
        shape(BF, 16, 24, 128),
        scratch=[pltpu.VMEM((24, wide), F32)],
        count=2,
        name="down",
    )(hidden, feedforward_down_weight)
    down = exchange(down, TP)
    return (residual + jnp.sum(down.astype(F32), axis=0)).astype(BF)


def solution(mesh):
    finer = Mesh(mesh.devices.reshape(4, 2, 2, 2, 4, 4), (*KV, *TP))
    placed = (
        P(None, KV),
        P(),
        P(KV, TP),
        P(KV, TP),
        P(KV, TP),
        P(KV, TP),
        P(),
        P(),
        P(),
        P(),
        P(TP, KV),
        P(),
        P(KV, TP),
        P(KV, TP),
        P(TP, KV),
        P(None, KV, TP),
        P(None, KV, TP),
        P(None, None, KV),
        P(None, TP, KV),
        P(),
    )
    return jax.shard_map(
        shards, mesh=finer, in_specs=placed, out_specs=P(None, KV), check_vma=False
    )
```

```python
import jax
import jax.numpy as jnp
from jax import lax
from jax.experimental import pallas as pl
from jax.experimental.pallas import tpu as pltpu
from jax.sharding import Mesh
from jax.sharding import PartitionSpec as P

D = 4096
KEY_CHANNELS = 128
DV = 256
GROUPS = 8
MEMBERS = 4
OWN = 6
Z = ("za", "zb", "zc")
KVL = ("zc", "core")
NEAR = ("zb", "zc", "core")
KV = (*Z, "core")
TP = ("tp_0", "tp_1")
NORM_EPSILON = 1e-06
BF = jnp.bfloat16
F32 = jnp.float32


BIG = 1e9
VMEM_LIMIT = 16 * 1024 * 1024


def exchange(array, axes):
    return lax.all_to_all(array, axes, split_axis=0, concat_axis=0, tiled=True)


def copies(array, size):
    return jnp.broadcast_to(array, (size, *array.shape))


def iota(shape, dim):
    return lax.broadcasted_iota(jnp.int32, shape, dim)


def dot(lhs, rhs, contract=((1,), (0,))):
    return lax.dot_general(lhs, rhs, (contract, ((), ())), preferred_element_type=F32)


def rounded(array):
    return array.astype(BF).astype(F32)


def log_gate(values):
    return (jnp.minimum(values, 0.0) - jnp.log(1.0 + jnp.exp(-jnp.abs(values)))) * 0.0625


def silu(values):
    return values / (1.0 + jnp.exp(-values))


def place_of():
    group, member = lax.axis_index(("za", "zb")), lax.axis_index(KVL)
    return group, member, group * MEMBERS + member


def kernel_call(kernel, outs, scratch=(), hbm=(), flops=1_000_000, count=0, name=None):
    specs = [
        pl.BlockSpec(memory_space=pltpu.HBM if i in hbm else pltpu.VMEM) for i in range(count)
    ]
    many = isinstance(outs, (tuple, list))
    call = pl.pallas_call(
        kernel,
        out_shape=outs,
        in_specs=specs,
        out_specs=[pl.BlockSpec(memory_space=pltpu.VMEM)] * len(outs)
        if many
        else pl.BlockSpec(memory_space=pltpu.VMEM),
        scratch_shapes=list(scratch),
        cost_estimate=pl.CostEstimate(flops=flops, bytes_accessed=1_000_000, transcendentals=0),
        compiler_params=pltpu.CompilerParams(vmem_limit_bytes=VMEM_LIMIT),
        name=name,
    )
    return lambda *args: call(
        *(
            pltpu.with_memory_space_constraint(a, pltpu.HBM) if i in hbm else a
            for i, a in enumerate(args)
        )
    )


def fetched(pairs, sems):
    moves = [pltpu.make_async_copy(src, dst, sems.at[i]) for i, (src, dst) in enumerate(pairs)]
    for move in moves:
        move.start()
    return moves


def spread_rows(decay_cols):
    stacked = jnp.concatenate([decay_cols] * 8, axis=0)
    owner = lax.shift_right_logical(iota((128, 128), 0), 4)
    blocks = [jnp.where(owner == m, stacked, 0.0) for m in range(8)]
    seq_row = iota((16, 128), 0) & 7
    ones = [(seq_row == m).astype(F32) for m in range(8)]
    return jnp.concatenate(blocks, axis=1).astype(BF), jnp.concatenate(ones, axis=1).astype(BF)


def gate_inputs(b, lowcache, extra, blocks, ones, pre, add):
    pre[...] = dot(lowcache[128 * b : 128 * b + 128, :], blocks, ((0,), (0,)))
    lines = jnp.concatenate([extra[8 * b + m] for m in range(8)], axis=0)
    high = rounded(lines)
    both = jnp.concatenate([high, lines - high], axis=0).astype(BF)
    add[...] = dot(both, ones, ((0,), (0,)))


def start_kernel(
    lengths_h,
    lowcache_h,
    decay_h,
    bias_h,
    extra_h,
    tokens_h,
    gain_h,
    low_h,
    query_h,
    key_h,
    value_h,
    outgate_h,
    send,
    lengths,
    lowcache,
    decay,
    bias,
    extra,
    tokens,
    gain,
    low_w,
    query_w,
    key_w,
    value_w,
    outgate_w,
    pre,
    sems,
):
    group, member, place = place_of()
    head = lax.axis_index(TP)
    head_lanes = pl.ds(pl.multiple_of(head * 128, 128), 128)
    place_lanes = pl.ds(pl.multiple_of(place * 128, 128), 128)
    moves = fetched(
        [
            (decay_h.at[:, head_lanes], decay),
            (lowcache_h, lowcache),
            (extra_h, extra),
            (bias_h, bias),
            (lengths_h, lengths),
            (tokens_h, tokens),
            (gain_h, gain),
            (low_h.at[:, place_lanes], low_w),
            (query_h, query_w),
            (key_h, key_w),
            (value_h, value_w),
            (outgate_h, outgate_w),
        ],
        sems,
    )
    start = place * 192
    ids = start + iota((192, 128), 0)
    for move in moves[:5]:
        move.wait()
    blocks = spread_rows(decay[...].astype(F32))[0]
    bias_row = bias[pl.ds(head, 1), :]
    line_ids = start + iota((1, 192), 1)
    for b in range(3):
        pre[...] = dot(lowcache[128 * b : 128 * b + 128, :], blocks, ((0,), (0,)))
        for m in range(8):
            s, lanes = 8 * b + m, slice(128 * m, 128 * m + 128)
            value = jnp.where(ids < lengths[s], pre[:, lanes] + bias_row, BIG)
            factor = (1.0 + jnp.exp(-jnp.abs(value))).reshape(24, 8, 128)
            while factor.shape[0] > 3:
                half = factor.shape[0] // 2
                factor = factor[:half] * factor[half:]
            factor = factor[0] * factor[1] * factor[2]
            below = jnp.sum(jnp.minimum(value, 0.0).reshape(24, 8, 128), axis=0)
            gate = jnp.sum(below - jnp.log(factor), axis=0, keepdims=True) * 0.0625
            line = jnp.where(line_ids < lengths[s], extra[s], 0.0)
            send[24 + s : 25 + s, :] = gate + jnp.sum(line, axis=1, keepdims=True)
    for move in moves[5:]:
        move.wait()
    tokens_f = tokens[...].astype(F32)
    scaled = (tokens_f * gain[pl.ds(place, 1), :]).astype(BF)
    send[:24, :] = dot(scaled, query_w[...])
    send[48:72, :] = dot(scaled, key_w[...])
    for i, weights in enumerate((value_w, outgate_w)):
        out, at = dot(scaled, weights[...]), 72 + 48 * i
        send[at : at + 24, :] = out[:, :128]
        send[at + 24 : at + 48, :] = out[:, 128:]
    low_t = low_w[...].astype(F32)
    low_t = jnp.concatenate([low_t] * OWN + [jnp.zeros((32, 128), F32)], axis=0).astype(BF)
    low = dot(scaled, low_t, ((1,), (1,)))
    squares = jnp.sum(tokens_f * tokens_f, axis=1, keepdims=True)
    lane, row = iota((24, 128), 1), iota((24, 128), 0)
    owner = sum((row >= OWN * r).astype(jnp.int32) for r in range(1, MEMBERS))
    slot = row - OWN * owner
    line = jnp.where(lax.shift_right_logical(lane, 4) == slot, low, 0.0)
    line = jnp.where(lane >= 96, 0.0, line)
    line = jnp.where(lane == 96 + slot, squares, line)
    for r in range(MEMBERS):
        at = slice(OWN * r, OWN * r + OWN)
        send[168 + r : 169 + r, :] = jnp.sum(line[at], axis=0, keepdims=True)
    send[172:, :] = jnp.zeros((4, 128), F32)


def first_kernel(both, send, near, held):
    core = lax.axis_index("core")
    held[...] = both[0] + both[1]
    near[...] = jnp.zeros_like(near)
    for r in range(MEMBERS):
        at = 24 + OWN * r
        near[r, :OWN, :] = jnp.where(core == 0, both[1, at : at + OWN, :], 0.0)

    def picked(start, size, step=OWN):
        low, high = held[start : start + size, :], held[start + step : start + step + size, :]
        return jnp.where(core == 0, low, high)

    for t in range(2):
        for a in range(3):
            query_pair = picked(12 * t + 2 * a, 2).astype(BF)
            total_pair = picked(24 + 12 * t + 2 * a, 2).astype(BF)
            for g in range(GROUPS):
                send[2 * g + t, a] = query_pair
                send[2 * g + t, 3 + a] = total_pair
        line = picked(168 + 2 * t, 1, 1)
        lane = iota((1, 128), 1)
        is_square = (lane >= 96) & (lane < 102)
        top = jnp.where(is_square, rounded(line), line)
        rest = jnp.where(is_square, line - rounded(line), 0.0)
        line = top + pltpu.roll(rest, OWN, 1)
        for g in range(GROUPS):
            s = 12 * t + min(g, OWN - 1)
            for a, lines in enumerate(
                (
                    (line, picked(48 + s, 1)),
                    (picked(72 + s, 1), picked(96 + s, 1)),
                    (picked(120 + s, 1), picked(144 + s, 1)),
                )
            ):
                send[2 * g + t, 6 + a] = jnp.concatenate(lines, axis=0).astype(BF)


def halves(row):
    return jnp.concatenate([row[:, :128], row[:, 128:]], axis=0).astype(BF)


def state_kernel(
    lengths_h,
    lowcache_h,
    decay_h,
    bias_h,
    extra_h,
    keys_h,
    values_h,
    state,
    lengths,
    lowcache,
    decay,
    bias,
    extra,
    keys,
    values,
    pre,
    add,
    rounded_gates,
    sems,
):
    _, _, place = place_of()
    head = lax.axis_index(TP)
    head_lanes = pl.ds(pl.multiple_of(head * 128, 128), 128)
    moves = fetched(
        [
            (decay_h.at[:, head_lanes], decay),
            (lowcache_h, lowcache),
            (extra_h, extra),
            (bias_h, bias),
            (lengths_h, lengths),
        ]
        + [
            (whole.at[8 * b : 8 * b + 8], part.at[8 * b : 8 * b + 8])
            for b in range(3)
            for whole, part in ((keys_h, keys), (values_h, values))
        ],
        sems,
    )
    later = (iota((192, 192), 1) > iota((192, 192), 0)).astype(F32).astype(BF)
    ids = place * 192 + iota((192, 128), 0)
    for move in moves[:5]:
        move.wait()
    blocks, ones = spread_rows(decay[...].astype(F32))
    bias_row = bias[pl.ds(head, 1), :]
    for b in range(3):
        gate_inputs(b, lowcache, extra, blocks, ones, pre, add)
        for m in range(8):
            lanes = slice(128 * m, 128 * m + 128)
            gate = log_gate(pre[:, lanes] + bias_row) + add[:, lanes]
            gate = jnp.where(ids < lengths[8 * b + m], gate, 0.0)
            rounded_gates[:, lanes] = gate.astype(BF)
        pre[...] = dot(later, rounded_gates[...])
        for move in moves[5 + 2 * b : 7 + 2 * b]:
            move.wait()
        for m in range(8):
            s, lanes = 8 * b + m, slice(128 * m, 128 * m + 128)
            weighted = keys[s].astype(F32) * jnp.exp(pre[:, lanes])
            weighted = jnp.where(ids < lengths[s], weighted, 0.0).astype(BF)
            state[128 * s : 128 * s + 128, :] = dot(weighted, values[s], ((0,), (0,))).astype(BF)


def query_kernel(got, decay_w, bias, ready, own_value, outgate, low_stack, held):
    group, member, place = place_of()
    head = lax.axis_index(TP)
    decay_cols = decay_w[:, pl.ds(pl.multiple_of(head * 128, 128), 128)].astype(F32)
    bias_row = bias[pl.ds(head, 1), :]
    stack = jnp.concatenate([decay_cols] * OWN + [jnp.zeros((32, 128), F32)], axis=0).astype(BF)

    def summed(a):
        return jnp.sum(got[:, a].astype(F32), axis=0)

    held[...] = jnp.zeros_like(held)
    for a in range(3):
        at = slice(2 * a, 2 * a + 2)
        held[2, at, :] = summed(a)
        beyond = jnp.zeros((2, 128), F32)
        own = jnp.zeros((2, 128), F32)
        for k in range(GROUPS):
            one, two = got[2 * k, 3 + a].astype(F32), got[2 * k + 1, 3 + a].astype(F32)
            beyond = beyond + jnp.where(k > group, one + two, 0.0)
            own = own + jnp.where(k == group, two, 0.0)
        held[0, at, :] = beyond + own
        held[1, at, :] = beyond
    mixed_pair = summed(6)
    line, key_sum = mixed_pair[0:1], mixed_pair[1:2]
    lane, row = iota((8, 128), 1), iota((8, 128), 0)
    wide = jnp.broadcast_to(line, (8, 128))
    square = jnp.sum(
        jnp.where((row < OWN) & ((lane == 96 + row) | (lane == 102 + row)), wide, 0.0),
        axis=1,
        keepdims=True,
    )
    inv = lax.rsqrt(square * (1.0 / D) + NORM_EPSILON)
    low = jnp.where((lax.shift_right_logical(lane, 4) == row) & (row < OWN), wide, 0.0)
    fresh = log_gate(dot((inv * low).astype(BF), stack) + bias_row)
    query = rounded(inv * held[2]) * KEY_CHANNELS ** (-0.5)
    for t in range(2):
        one = query * jnp.exp(fresh + held[t])
        ready[2 * t] = one
        ready[2 * t + 1] = one
    is_own = row == group
    own_query = jnp.sum(jnp.where(is_own, query, 0.0), axis=0, keepdims=True)
    own_inv = jnp.sum(jnp.where(is_own[:, :1], inv, 0.0), axis=0, keepdims=True)
    own = jnp.sum(own_query * rounded(own_inv * key_sum), axis=1, keepdims=True)
    pair = own * rounded(own_inv * summed(7))
    own_value[:, :128], own_value[:, 128:] = pair[0:1], pair[1:2]
    pair = rounded(own_inv * summed(8))
    outgate[:, :128], outgate[:, 128:] = pair[0:1], pair[1:2]


def heads_kernel(whole, near, state, own_value, outgate, send):
    group, member, place = place_of()
    query = (whole[...] * jnp.exp(near[...])).reshape(32, 128)
    high = rounded(query)
    both = jnp.concatenate([high, query - high], axis=0)
    row = iota((64, 128), 0) & 31
    spread = jnp.concatenate(
        [
            jnp.where(row == 8 * (s // OWN) + s % OWN, both, 0.0).astype(BF)
            for s in range(24)
        ],
        axis=1,
    )
    part = dot(spread, state[...])
    part = part[:32] + part[32:]
    row = iota((32, DV), 0)
    part = part + jnp.where(row == 8 * member + group, own_value[...], 0.0)
    send[...] = jnp.where(row == 8 * member + OWN, outgate[...], part)


def sums_kernel(both, send, held):
    core = lax.axis_index("core")
    held[...] = both[0] + both[1]
    for t in range(2):
        block = held[pl.ds(pl.multiple_of(8 * (2 * t + core), 8), 8), :]
        for k in range(OWN + 1):
            pair = halves(block[k : k + 1])
            for g in range(GROUPS):
                send[2 * g + t, k] = pair


def gating_kernel(back, gain, send, mixed_rows, gate_rows):
    group, member, place = place_of()
    mixed_rows[...] = jnp.zeros_like(mixed_rows)
    gate_rows[...] = jnp.zeros_like(gate_rows)
    for k in range(OWN):
        pair = jnp.sum(back[:, k].astype(F32), axis=0)
        mixed_rows[k : k + 1, :128], mixed_rows[k : k + 1, 128:] = pair[0:1], pair[1:2]
        pair = back[2 * k + lax.shift_right_logical(member, 1), OWN].astype(F32)
        gate_rows[k : k + 1, :128], gate_rows[k : k + 1, 128:] = pair[0:1], pair[1:2]
    mixed = mixed_rows[...]
    mean_sq = jnp.sum(mixed * mixed, axis=1, keepdims=True) * (1.0 / DV)
    gated = mixed * lax.rsqrt(mean_sq + NORM_EPSILON) * gain[...] * silu(gate_rows[...])
    gated = gated.astype(BF)
    send[...] = gated


def output_kernel(gated, packed, send, held):
    for c in range(2):
        weights = in_lanes(packed.at[c], 520, (88, 88, 80)).astype(BF)
        rows = dot(gated[...].reshape(16, DV), weights)
        for t in range(2):
            at = 2 * OWN * c + OWN * t
            held[at : at + OWN, :] = rows[8 * t : 8 * t + OWN]
    rows = held[...].astype(BF)
    for h in range(32):
        send[h] = rows


def pack_kernel(gate_w, up_w, output_w, tokens, send):
    half = gate_w.shape[1] // 2
    zeros = jnp.zeros((128, send.shape[1] - half), F32)
    for i, weights in enumerate((gate_w, up_w)):
        whole = weights[...].astype(F32)
        for c in range(2):
            part = whole[:, half * c : half * c + half]
            at = 256 * c + 128 * i
            send[at : at + 128, :] = jnp.concatenate([part, zeros], axis=1).astype(BF)
    send[512:608, :] = jnp.zeros((96, send.shape[1]), BF)
    for b in range(3):
        lanes = slice(128 * b, 128 * b + 128)
        send[512:520, lanes] = tokens[8 * b : 8 * b + 8, :]
        count = min(88, 256 - 88 * b)
        send[520 : 520 + count, lanes] = output_w[88 * b : 88 * b + count, :]


def in_lanes(packed, start, sizes):
    return jnp.concatenate(
        [
            packed[start : start + size, 128 * b : 128 * b + 128].astype(F32)
            for b, size in enumerate(sizes)
        ],
        axis=0,
    )


def wide_kernel(rows, gain, packed, send, residual, held):
    core = lax.axis_index("core")
    _, _, place = place_of()
    gate = up = square = 0.0
    for source in range(2):
        part = jnp.sum(rows[16 * source : 16 * source + 16].astype(F32), axis=0)
        for c in range(2):
            for t in range(2):
                at, to = 2 * OWN * c + OWN * t, 2 * OWN * t + OWN * source
                held[c, to : to + OWN, :] = part[at : at + OWN]
    for c in range(2):
        total = held[c] + in_lanes(packed.at[c], 512, (8, 8, 8))

        @pl.when(core == c)
        def _():
            residual[...] = total

        scaled = (total * gain[pl.ds(place - core + c, 1), :]).astype(BF)
        square += jnp.sum(total * total, axis=1, keepdims=True)
        gate += dot(scaled, packed[c, pl.ds(pl.multiple_of(256 * core, 256), 128), :])
        up += dot(scaled, packed[c, pl.ds(pl.multiple_of(256 * core + 128, 128), 128), :])
    high = rounded(square)
    spare = iota(gate.shape, 1) == gate.shape[1] - 1
    gate = jnp.where(spare, high, gate)
    up = jnp.where(spare, square - high, up)
    for s in range(24):
        pair = jnp.concatenate([gate[s : s + 1], up[s : s + 1]], axis=0).astype(BF)
        for z in range(4):
            send[4 * z + s // OWN, s % OWN] = pair


def hidden_kernel(got, send, gates, ups):
    wide = send.shape[2]
    gates[...] = jnp.zeros_like(gates)
    ups[...] = jnp.zeros_like(ups)
    for k in range(OWN):
        pair = jnp.sum(got[:, k].astype(F32), axis=0)
        gates[k : k + 1, :] = pair[0:1]
        ups[k : k + 1, :] = pair[1:2]
    gate, up = gates[...], ups[...]
    square = gate[:, wide - 1 :] + up[:, wide - 1 :]
    inv = lax.rsqrt(square * (1.0 / D) + NORM_EPSILON)
    hidden = (silu(inv * gate) * (inv * up)).astype(BF)
    for j in range(8):
        send[j] = hidden


def down_kernel(got, down_w, send, held):
    half = down_w.shape[0] // 2
    total = 0.0
    for c in range(2):
        for z in range(4):
            held[OWN * z : OWN * z + OWN, :] = got[2 * z + c].astype(F32)[:OWN]
        total += dot(held[...].astype(BF)[:, :half], down_w[half * c : half * c + half, :])
    total = total.astype(BF)
    for h in range(16):
        send[h] = total


def shape(dtype, *dims):
    return jax.ShapeDtypeStruct(dims, dtype)


def shards(
    tokens,
    attention_norm_gain,
    query_weight,
    key_weight,
    value_weight,
    output_gate_weight,
    lowrank_weight,
    decay_weight,
    decay_preact_bias,
    head_norm_gain,
    output_weight,
    feedforward_norm_gain,
    feedforward_gate_weight,
    feedforward_up_weight,
    feedforward_down_weight,
    past_key_cache,
    past_value_cache,
    past_lowrank_cache,
    head_extra_decay,
    lengths,
):
    bias = decay_preact_bias.reshape(16, 128)
    lowcache = past_lowrank_cache.reshape(384, 192)
    gate_scratch = [
        pltpu.SMEM((24,), jnp.int32),
        pltpu.VMEM((384, 192), BF),
        pltpu.VMEM((16, 128), BF),
        pltpu.VMEM((16, 128), F32),
        pltpu.VMEM((24, 1, 192), F32),
    ]
    first = kernel_call(
        start_kernel,
        shape(F32, 176, 128),
        scratch=gate_scratch
        + [
            pltpu.VMEM((24, 128), BF),
            pltpu.VMEM((32, 128), F32),
            pltpu.VMEM((16, 128), BF),
            pltpu.VMEM((128, 128), BF),
            pltpu.VMEM((128, 128), BF),
            pltpu.VMEM((128, DV), BF),
            pltpu.VMEM((128, DV), BF),
            pltpu.VMEM((192, 1024), F32),
            pltpu.SemaphoreType.DMA((12,)),
        ],
        count=12,
        hbm=range(12),
        name="start",
    )(
        lengths,
        lowcache,
        decay_weight,
        bias,
        head_extra_decay,
        tokens,
        attention_norm_gain.reshape(32, 128),
        lowrank_weight.T,
        query_weight,
        key_weight,
        value_weight,
        output_gate_weight,
    )
    first, near = kernel_call(
        first_kernel,
        (shape(BF, 16, 9, 2, 128), shape(F32, MEMBERS, 8, 128)),
        scratch=[pltpu.VMEM((176, 128), F32)],
        count=1,
        name="first",
    )(lax.all_gather(first, "core"))
    late_cache, first = lax.optimization_barrier((lowcache, first))
    got = exchange(first, Z)
    state = kernel_call(
        state_kernel,
        pltpu.VMEM((3072, DV), BF),
        scratch=gate_scratch
        + [
            pltpu.VMEM((24, 192, 128), BF),
            pltpu.VMEM((24, 192, DV), BF),
            pltpu.VMEM((192, 1024), F32),
            pltpu.VMEM((192, 1024), F32),
            pltpu.VMEM((192, 1024), BF),
            pltpu.SemaphoreType.DMA((11,)),
        ],
        count=7,
        hbm=range(7),
        flops=20_000_000_000,
        name="state",
    )(
        lengths,
        late_cache,
        decay_weight,
        bias,
        head_extra_decay,
        past_key_cache,
        past_value_cache,
    )
    got, state = lax.optimization_barrier((got, state))
    ready, own_value, outgate = kernel_call(
        query_kernel,
        (shape(F32, MEMBERS, 8, 128), shape(F32, 1, DV), shape(F32, 1, DV)),
        scratch=[pltpu.VMEM((8, 128), F32), pltpu.VMEM((3, 8, 128), F32)],
        count=3,
        name="query",
    )(got, decay_weight, bias)
    whole = exchange(ready, KVL)
    part = kernel_call(heads_kernel, shape(F32, 32, DV), count=5, name="heads")(
        whole, near, state, own_value, outgate
    )
    second = kernel_call(
        sums_kernel,
        shape(BF, 16, 7, 2, 128),
        scratch=[pltpu.VMEM((32, DV), F32)],
        count=1,
        name="sums",
    )(lax.all_gather(part, "core"))
    gate_w, up_w, output_w, second = lax.optimization_barrier(
        (feedforward_gate_weight, feedforward_up_weight, output_weight, second)
    )
    units = feedforward_gate_weight.shape[1]
    wide = -(-(units // 2 + 1) // 128) * 128
    packed = kernel_call(pack_kernel, shape(BF, 608, wide), count=4, name="pack")(
        gate_w, up_w, output_w, tokens
    )
    packed = lax.all_gather(packed, "core")
    back = exchange(second, Z)
    back, packed = lax.optimization_barrier((back, packed))
    gated = kernel_call(
        gating_kernel,
        shape(BF, 8, DV),
        scratch=[pltpu.VMEM((8, DV), F32), pltpu.VMEM((8, DV), F32)],
        count=2,
        name="gating",
    )(back, head_norm_gain.reshape(1, DV))
    gated = lax.all_gather(gated, "zc")
    rows = kernel_call(
        output_kernel,
        shape(BF, 32, 24, 128),
        scratch=[pltpu.VMEM((24, 128), F32)],
        count=2,
        name="output",
    )(gated, packed)
    rows = exchange(rows, ("core", *TP))
    third, residual = kernel_call(
        wide_kernel,
        (shape(BF, 16, OWN, 2, wide), shape(F32, 24, 128)),
        scratch=[pltpu.VMEM((2, 24, 128), F32)],
        count=3,
        name="wide",
    )(rows, feedforward_norm_gain.reshape(32, 128), packed)
    third = exchange(third, Z)
    hidden = kernel_call(
        hidden_kernel,
        shape(BF, 8, 8, wide),
        scratch=[pltpu.VMEM((8, wide), F32)] * 2,
        count=1,
        name="hidden",
    )(third)
    hidden = exchange(hidden, NEAR)
    down = kernel_call(
        down_kernel,
        shape(BF, 16, 24, 128),
        scratch=[pltpu.VMEM((24, wide), F32)],
        count=2,
        name="down",
    )(hidden, feedforward_down_weight)
    down = exchange(down, TP)
    return (residual + jnp.sum(down.astype(F32), axis=0)).astype(BF)


def solution(mesh):
    finer = Mesh(mesh.devices.reshape(4, 2, 2, 2, 4, 4), (*KV, *TP))
    placed = (
        P(None, KV),
        P(),
        P(KV, TP),
        P(KV, TP),
        P(KV, TP),
        P(KV, TP),
        P(),
        P(),
        P(),
        P(),
        P(TP, KV),
        P(),
        P(KV, TP),
        P(KV, TP),
        P(TP, KV),
        P(None, KV, TP),
        P(None, KV, TP),
        P(None, None, KV),
        P(None, TP, KV),
        P(),
    )
    return jax.shard_map(
        shards, mesh=finer, in_specs=placed, out_specs=P(None, KV), check_vma=False
    )
```

```python
import jax
import jax.numpy as jnp
from jax import lax
from jax.experimental import pallas as pl
from jax.experimental.pallas import tpu as pltpu
from jax.sharding import Mesh
from jax.sharding import PartitionSpec as P

D = 4096
KEY_CHANNELS = 128
DV = 256
GROUPS = 8
MEMBERS = 4
OWN = 6
Z = ("za", "zb", "zc")
KVL = ("zc", "core")
NEAR = ("zb", "zc", "core")
KV = (*Z, "core")
TP = ("tp_0", "tp_1")
NORM_EPSILON = 1e-06
BF = jnp.bfloat16
F32 = jnp.float32


BIG = 1e9
HALF = 12
VMEM_LIMIT = 16 * 1024 * 1024


def exchange(array, axes):
    return lax.all_to_all(array, axes, split_axis=0, concat_axis=0, tiled=True)


def copies(array, size):
    return jnp.broadcast_to(array, (size, *array.shape))


def iota(shape, dim):
    return lax.broadcasted_iota(jnp.int32, shape, dim)


def dot(lhs, rhs, contract=((1,), (0,))):
    return lax.dot_general(lhs, rhs, (contract, ((), ())), preferred_element_type=F32)


def rounded(array):
    return array.astype(BF).astype(F32)


def log_gate(values):
    return (jnp.minimum(values, 0.0) - jnp.log(1.0 + jnp.exp(-jnp.abs(values)))) * 0.0625


def silu(values):
    return values / (1.0 + jnp.exp(-values))


def place_of():
    group, member = lax.axis_index(("za", "zb")), lax.axis_index(KVL)
    return group, member, group * MEMBERS + member


def kernel_call(kernel, outs, scratch=(), hbm=(), flops=1_000_000, count=0, name=None):
    specs = [
        pl.BlockSpec(memory_space=pltpu.HBM if i in hbm else pltpu.VMEM) for i in range(count)
    ]
    many = isinstance(outs, (tuple, list))
    call = pl.pallas_call(
        kernel,
        out_shape=outs,
        in_specs=specs,
        out_specs=[pl.BlockSpec(memory_space=pltpu.VMEM)] * len(outs)
        if many
        else pl.BlockSpec(memory_space=pltpu.VMEM),
        scratch_shapes=list(scratch),
        cost_estimate=pl.CostEstimate(flops=flops, bytes_accessed=1_000_000, transcendentals=0),
        compiler_params=pltpu.CompilerParams(vmem_limit_bytes=VMEM_LIMIT),
        name=name,
    )
    return lambda *args: call(
        *(
            pltpu.with_memory_space_constraint(a, pltpu.HBM) if i in hbm else a
            for i, a in enumerate(args)
        )
    )


def fetched(pairs, sems):
    moves = [pltpu.make_async_copy(src, dst, sems.at[i]) for i, (src, dst) in enumerate(pairs)]
    for move in moves:
        move.start()
    return moves


def spread_rows(decay_cols):
    stacked = jnp.concatenate([decay_cols] * 8, axis=0)
    owner = lax.shift_right_logical(iota((128, 128), 0), 4)
    blocks = [jnp.where(owner == m, stacked, 0.0) for m in range(8)]
    seq_row = iota((16, 128), 0) & 7
    ones = [(seq_row == m).astype(F32) for m in range(8)]
    return jnp.concatenate(blocks, axis=1).astype(BF), jnp.concatenate(ones, axis=1).astype(BF)


def gate_inputs(b, lowcache, extra, blocks, ones, pre, add):
    pre[...] = dot(lowcache[128 * b : 128 * b + 128, :], blocks, ((0,), (0,)))
    lines = jnp.concatenate([extra[8 * b + m] for m in range(8)], axis=0)
    high = rounded(lines)
    both = jnp.concatenate([high, lines - high], axis=0).astype(BF)
    add[...] = dot(both, ones, ((0,), (0,)))


def start_kernel(
    lengths_h,
    lowcache_h,
    decay_h,
    bias_h,
    extra_h,
    tokens_h,
    gain_h,
    low_h,
    query_h,
    key_h,
    value_h,
    outgate_h,
    send,
    lengths,
    lowcache,
    decay,
    bias,
    extra,
    tokens,
    gain,
    low_w,
    query_w,
    key_w,
    value_w,
    outgate_w,
    pre,
    sems,
):
    group, member, place = place_of()
    head = lax.axis_index(TP)
    head_lanes = pl.ds(pl.multiple_of(head * 128, 128), 128)
    place_lanes = pl.ds(pl.multiple_of(place * 128, 128), 128)
    moves = fetched(
        [
            (decay_h.at[:, head_lanes], decay),
            (lowcache_h, lowcache),
            (extra_h, extra),
            (bias_h, bias),
            (lengths_h, lengths),
            (tokens_h, tokens),
            (gain_h, gain),
            (low_h.at[:, place_lanes], low_w),
            (query_h, query_w),
            (key_h, key_w),
            (value_h, value_w),
            (outgate_h, outgate_w),
        ],
        sems,
    )
    start = place * 192
    ids = start + iota((192, 128), 0)
    for move in moves[:5]:
        move.wait()
    blocks = spread_rows(decay[...].astype(F32))[0]
    bias_row = bias[pl.ds(head, 1), :]
    line_ids = start + iota((1, 192), 1)
    for b in range(3):
        pre[...] = dot(lowcache[128 * b : 128 * b + 128, :], blocks, ((0,), (0,)))
        for m in range(8):
            s, lanes = 8 * b + m, slice(128 * m, 128 * m + 128)
            value = jnp.where(ids < lengths[s], pre[:, lanes] + bias_row, BIG)
            factor = (1.0 + jnp.exp(-jnp.abs(value))).reshape(24, 8, 128)
            while factor.shape[0] > 3:
                half = factor.shape[0] // 2
                factor = factor[:half] * factor[half:]
            factor = factor[0] * factor[1] * factor[2]
            below = jnp.sum(jnp.minimum(value, 0.0).reshape(24, 8, 128), axis=0)
            gate = jnp.sum(below - jnp.log(factor), axis=0, keepdims=True) * 0.0625
            line = jnp.where(line_ids < lengths[s], extra[s], 0.0)
            send[24 + s : 25 + s, :] = gate + jnp.sum(line, axis=1, keepdims=True)
    for move in moves[5:]:
        move.wait()
    tokens_f = tokens[...].astype(F32)
    scaled = (tokens_f * gain[pl.ds(place, 1), :]).astype(BF)
    send[:24, :] = dot(scaled, query_w[...])
    send[48:72, :] = dot(scaled, key_w[...])
    for i, weights in enumerate((value_w, outgate_w)):
        out, at = dot(scaled, weights[...]), 72 + 48 * i
        send[at : at + 24, :] = out[:, :128]
        send[at + 24 : at + 48, :] = out[:, 128:]
    low_t = low_w[...].astype(F32)
    low_t = jnp.concatenate([low_t] * OWN + [jnp.zeros((32, 128), F32)], axis=0).astype(BF)
    low = dot(scaled, low_t, ((1,), (1,)))
    squares = jnp.sum(tokens_f * tokens_f, axis=1, keepdims=True)
    lane, row = iota((24, 128), 1), iota((24, 128), 0)
    owner = sum((row >= OWN * r).astype(jnp.int32) for r in range(1, MEMBERS))
    slot = row - OWN * owner
    line = jnp.where(lax.shift_right_logical(lane, 4) == slot, low, 0.0)
    line = jnp.where(lane >= 96, 0.0, line)
    line = jnp.where(lane == 96 + slot, squares, line)
    for r in range(MEMBERS):
        at = slice(OWN * r, OWN * r + OWN)
        send[168 + r : 169 + r, :] = jnp.sum(line[at], axis=0, keepdims=True)
    send[172:, :] = jnp.zeros((4, 128), F32)


def first_kernel(both, send, near, held):
    core = lax.axis_index("core")
    held[...] = both[0] + both[1]
    near[...] = jnp.zeros_like(near)
    for c in range(2):
        at = 24 + HALF * c
        near[c, :HALF, :] = jnp.where(core == 0, both[1, at : at + HALF, :], 0.0)

    def picked(start, size, step=HALF):
        low, high = held[start : start + size, :], held[start + step : start + step + size, :]
        return jnp.where(core == 0, low, high)

    lines = picked(168, 2, 2)
    lane = iota((2, 128), 1)
    is_square = (lane >= 96) & (lane < 102)
    top = jnp.where(is_square, rounded(lines), lines)
    rest = jnp.where(is_square, lines - rounded(lines), 0.0)
    shared = [picked(2 * a, 2) for a in range(6)] + [picked(24 + 2 * a, 2) for a in range(6)]
    shared.append(top + pltpu.roll(rest, OWN, 1))
    for a, pair in enumerate(shared):
        pair = pair.astype(BF)
        for z in range(16):
            send[z, a] = pair
    for z in range(16):
        s = min(z, HALF - 1)
        for a, pair in enumerate(
            (
                (picked(48 + s, 1), jnp.zeros((1, 128), F32)),
                (picked(72 + s, 1), picked(96 + s, 1)),
                (picked(120 + s, 1), picked(144 + s, 1)),
            )
        ):
            send[z, 13 + a] = jnp.concatenate(pair, axis=0).astype(BF)


def halves(row):
    return jnp.concatenate([row[:, :128], row[:, 128:]], axis=0).astype(BF)


def state_kernel(
    lengths_h,
    lowcache_h,
    decay_h,
    bias_h,
    extra_h,
    keys_h,
    values_h,
    state,
    lengths,
    lowcache,
    decay,
    bias,
    extra,
    keys,
    values,
    pre,
    add,
    rounded_gates,
    sems,
):
    _, _, place = place_of()
    head = lax.axis_index(TP)
    head_lanes = pl.ds(pl.multiple_of(head * 128, 128), 128)
    moves = fetched(
        [
            (decay_h.at[:, head_lanes], decay),
            (lowcache_h, lowcache),
            (extra_h, extra),
            (bias_h, bias),
            (lengths_h, lengths),
        ]
        + [
            (whole.at[8 * b : 8 * b + 8], part.at[8 * b : 8 * b + 8])
            for b in range(3)
            for whole, part in ((keys_h, keys), (values_h, values))
        ],
        sems,
    )
    later = (iota((192, 192), 1) > iota((192, 192), 0)).astype(F32).astype(BF)
    ids = place * 192 + iota((192, 128), 0)
    for move in moves[:5]:
        move.wait()
    blocks, ones = spread_rows(decay[...].astype(F32))
    bias_row = bias[pl.ds(head, 1), :]
    for b in range(3):
        gate_inputs(b, lowcache, extra, blocks, ones, pre, add)
        for m in range(8):
            lanes = slice(128 * m, 128 * m + 128)
            gate = log_gate(pre[:, lanes] + bias_row) + add[:, lanes]
            gate = jnp.where(ids < lengths[8 * b + m], gate, 0.0)
            rounded_gates[:, lanes] = gate.astype(BF)
        pre[...] = dot(later, rounded_gates[...])
        for move in moves[5 + 2 * b : 7 + 2 * b]:
            move.wait()
        for m in range(8):
            s, lanes = 8 * b + m, slice(128 * m, 128 * m + 128)
            weighted = keys[s].astype(F32) * jnp.exp(pre[:, lanes])
            weighted = jnp.where(ids < lengths[s], weighted, 0.0).astype(BF)
            state[128 * s : 128 * s + 128, :] = dot(weighted, values[s], ((0,), (0,))).astype(BF)


def query_kernel(got, decay_w, bias, ready, own_value, outgate, later, query_sum):
    _, _, place = place_of()
    level = lax.shift_right_logical(place, 1)
    head = lax.axis_index(TP)
    decay_cols = decay_w[:, pl.ds(pl.multiple_of(head * 128, 128), 128)].astype(F32)
    bias_row = bias[pl.ds(head, 1), :]
    stack = jnp.concatenate([decay_cols] * OWN + [jnp.zeros((32, 128), F32)], axis=0).astype(BF)

    def summed(a):
        return jnp.sum(got[:, a].astype(F32), axis=0)

    later[...] = jnp.zeros_like(later)
    query_sum[...] = jnp.zeros_like(query_sum)
    for a in range(6):
        at = slice(2 * a, 2 * a + 2)
        query_sum[at, :] = summed(a)
        beyond = jnp.zeros((2, 128), F32)
        for z in range(16):
            beyond = beyond + jnp.where(z > level, got[z, 6 + a].astype(F32), 0.0)
        later[at, :] = beyond
    lines = summed(12)
    lane, row = iota((16, 128), 1), iota((16, 128), 0)
    wide = jnp.where(row < OWN, lines[0:1], lines[1:2])
    slot = jnp.where(row < OWN, row, row - OWN)
    held = row < HALF
    square = jnp.sum(
        jnp.where(held & ((lane == 96 + slot) | (lane == 102 + slot)), wide, 0.0),
        axis=1,
        keepdims=True,
    )
    inv = lax.rsqrt(square * (1.0 / D) + NORM_EPSILON)
    low = jnp.where((lax.shift_right_logical(lane, 4) == slot) & held, wide, 0.0)
    fresh = log_gate(dot((inv * low).astype(BF), stack) + bias_row)
    query = rounded(inv * query_sum[...]) * KEY_CHANNELS ** (-0.5)
    ready[...] = query * jnp.exp(fresh + later[...])
    is_own = row == level
    own_query = jnp.sum(jnp.where(is_own, query, 0.0), axis=0, keepdims=True)
    own_inv = jnp.sum(jnp.where(is_own[:, :1], inv, 0.0), axis=0, keepdims=True)
    key_new = rounded(own_inv * summed(13)[0:1])
    own = jnp.sum(own_query * key_new, axis=1, keepdims=True)
    pair = own * rounded(own_inv * summed(14))
    own_value[:, :128], own_value[:, 128:] = pair[0:1], pair[1:2]
    pair = rounded(own_inv * summed(15))
    outgate[:, :128], outgate[:, 128:] = pair[0:1], pair[1:2]


def heads_kernel(whole, near, state, own_value, outgate, send):
    core = lax.axis_index("core")
    _, _, place = place_of()
    query = (whole[...] * jnp.exp(near[...])).reshape(32, 128)
    high = rounded(query)
    both = jnp.concatenate([high, query - high], axis=0)
    row = iota((64, 128), 0) & 31
    spread = jnp.concatenate(
        [
            jnp.where(row == 16 * (s // HALF) + s % HALF, both, 0.0).astype(BF)
            for s in range(24)
        ],
        axis=1,
    )
    part = dot(spread, state[...])
    part = part[:32] + part[32:]
    row = iota((32, DV), 0) - 16 * core
    part = part + jnp.where(row == lax.shift_right_logical(place, 1), own_value[...], 0.0)
    send[...] = jnp.where(row == HALF, outgate[...], part)


def sums_kernel(both, send, held):
    core = lax.axis_index("core")
    held[...] = both[0] + both[1]
    block = held[pl.ds(pl.multiple_of(16 * core, 16), 16), :]
    for k in range(HALF + 1):
        pair = halves(block[k : k + 1])
        for z in range(16):
            send[z, k] = pair


def gating_kernel(back, gain, packed, send, mixed_rows, gate_rows, held):
    mixed_rows[...] = jnp.zeros_like(mixed_rows)
    gate_rows[...] = jnp.zeros_like(gate_rows)
    for k in range(HALF):
        pair = jnp.sum(back[:, k].astype(F32), axis=0)
        mixed_rows[k : k + 1, :128], mixed_rows[k : k + 1, 128:] = pair[0:1], pair[1:2]
        pair = back[k, HALF].astype(F32)
        gate_rows[k : k + 1, :128], gate_rows[k : k + 1, 128:] = pair[0:1], pair[1:2]
    mixed = mixed_rows[...]
    mean_sq = jnp.sum(mixed * mixed, axis=1, keepdims=True) * (1.0 / DV)
    gated = mixed * lax.rsqrt(mean_sq + NORM_EPSILON) * gain[...] * silu(gate_rows[...])
    gated = gated.astype(BF)
    for c in range(2):
        weights = in_lanes(packed.at[c], 520, (88, 88, 80)).astype(BF)
        held[HALF * c : HALF * c + HALF, :] = dot(gated, weights)[:HALF]
    rows = held[...].astype(BF)
    for h in range(32):
        send[h] = rows


def pack_kernel(gate_w, up_w, output_w, tokens, send):
    half = gate_w.shape[1] // 2
    zeros = jnp.zeros((128, send.shape[1] - half), F32)
    for i, weights in enumerate((gate_w, up_w)):
        whole = weights[...].astype(F32)
        for c in range(2):
            part = whole[:, half * c : half * c + half]
            at = 256 * c + 128 * i
            send[at : at + 128, :] = jnp.concatenate([part, zeros], axis=1).astype(BF)
    send[512:608, :] = jnp.zeros((96, send.shape[1]), BF)
    for b in range(3):
        lanes = slice(128 * b, 128 * b + 128)
        send[512:520, lanes] = tokens[8 * b : 8 * b + 8, :]
        count = min(88, 256 - 88 * b)
        send[520 : 520 + count, lanes] = output_w[88 * b : 88 * b + count, :]


def in_lanes(packed, start, sizes):
    return jnp.concatenate(
        [
            packed[start : start + size, 128 * b : 128 * b + 128].astype(F32)
            for b, size in enumerate(sizes)
        ],
        axis=0,
    )


def wide_kernel(rows, gain, packed, send, residual, held):
    core = lax.axis_index("core")
    _, _, place = place_of()
    gate = up = square = 0.0
    for source in range(2):
        part = jnp.sum(rows[16 * source : 16 * source + 16].astype(F32), axis=0)
        for c in range(2):
            held[c, HALF * source : HALF * source + HALF, :] = part[HALF * c : HALF * c + HALF]
    for c in range(2):
        total = held[c] + in_lanes(packed.at[c], 512, (8, 8, 8))

        @pl.when(core == c)
        def _():
            residual[...] = total

        scaled = (total * gain[pl.ds(place - core + c, 1), :]).astype(BF)
        square += jnp.sum(total * total, axis=1, keepdims=True)
        gate += dot(scaled, packed[c, pl.ds(pl.multiple_of(256 * core, 256), 128), :])
        up += dot(scaled, packed[c, pl.ds(pl.multiple_of(256 * core + 128, 128), 128), :])
    high = rounded(square)
    spare = iota(gate.shape, 1) == gate.shape[1] - 1
    gate = jnp.where(spare, high, gate)
    up = jnp.where(spare, square - high, up)
    for s in range(24):
        pair = jnp.concatenate([gate[s : s + 1], up[s : s + 1]], axis=0).astype(BF)
        for z in range(4):
            send[4 * z + s // OWN, s % OWN] = pair


def hidden_kernel(got, send, gates, ups):
    wide = send.shape[2]
    gates[...] = jnp.zeros_like(gates)
    ups[...] = jnp.zeros_like(ups)
    for k in range(OWN):
        pair = jnp.sum(got[:, k].astype(F32), axis=0)
        gates[k : k + 1, :] = pair[0:1]
        ups[k : k + 1, :] = pair[1:2]
    gate, up = gates[...], ups[...]
    square = gate[:, wide - 1 :] + up[:, wide - 1 :]
    inv = lax.rsqrt(square * (1.0 / D) + NORM_EPSILON)
    hidden = (silu(inv * gate) * (inv * up)).astype(BF)
    for j in range(8):
        send[j] = hidden


def down_kernel(got, down_w, send, held):
    half = down_w.shape[0] // 2
    total = 0.0
    for c in range(2):
        for z in range(4):
            held[OWN * z : OWN * z + OWN, :] = got[2 * z + c].astype(F32)[:OWN]
        total += dot(held[...].astype(BF)[:, :half], down_w[half * c : half * c + half, :])
    total = total.astype(BF)
    for h in range(16):
        send[h] = total


def shape(dtype, *dims):
    return jax.ShapeDtypeStruct(dims, dtype)


def shards(
    tokens,
    attention_norm_gain,
    query_weight,
    key_weight,
    value_weight,
    output_gate_weight,
    lowrank_weight,
    decay_weight,
    decay_preact_bias,
    head_norm_gain,
    output_weight,
    feedforward_norm_gain,
    feedforward_gate_weight,
    feedforward_up_weight,
    feedforward_down_weight,
    past_key_cache,
    past_value_cache,
    past_lowrank_cache,
    head_extra_decay,
    lengths,
):
    bias = decay_preact_bias.reshape(16, 128)
    lowcache = past_lowrank_cache.reshape(384, 192)
    gate_scratch = [
        pltpu.SMEM((24,), jnp.int32),
        pltpu.VMEM((384, 192), BF),
        pltpu.VMEM((16, 128), BF),
        pltpu.VMEM((16, 128), F32),
        pltpu.VMEM((24, 1, 192), F32),
    ]
    first = kernel_call(
        start_kernel,
        shape(F32, 176, 128),
        scratch=gate_scratch
        + [
            pltpu.VMEM((24, 128), BF),
            pltpu.VMEM((32, 128), F32),
            pltpu.VMEM((16, 128), BF),
            pltpu.VMEM((128, 128), BF),
            pltpu.VMEM((128, 128), BF),
            pltpu.VMEM((128, DV), BF),
            pltpu.VMEM((128, DV), BF),
            pltpu.VMEM((192, 1024), F32),
            pltpu.SemaphoreType.DMA((12,)),
        ],
        count=12,
        hbm=range(12),
        name="start",
    )(
        lengths,
        lowcache,
        decay_weight,
        bias,
        head_extra_decay,
        tokens,
        attention_norm_gain.reshape(32, 128),
        lowrank_weight.T,
        query_weight,
        key_weight,
        value_weight,
        output_gate_weight,
    )
    first, near = kernel_call(
        first_kernel,
        (shape(BF, 16, 16, 2, 128), shape(F32, 2, 16, 128)),
        scratch=[pltpu.VMEM((176, 128), F32)],
        count=1,
        name="first",
    )(lax.all_gather(first, "core"))
    late_cache, first = lax.optimization_barrier((lowcache, first))
    got = exchange(first, Z)
    state = kernel_call(
        state_kernel,
        pltpu.VMEM((3072, DV), BF),
        scratch=gate_scratch
        + [
            pltpu.VMEM((24, 192, 128), BF),
            pltpu.VMEM((24, 192, DV), BF),
            pltpu.VMEM((192, 1024), F32),
            pltpu.VMEM((192, 1024), F32),
            pltpu.VMEM((192, 1024), BF),
            pltpu.SemaphoreType.DMA((11,)),
        ],
        count=7,
        hbm=range(7),
        flops=20_000_000_000,
        name="state",
    )(
        lengths,
        late_cache,
        decay_weight,
        bias,
        head_extra_decay,
        past_key_cache,
        past_value_cache,
    )
    gate_w, up_w, output_w, state = lax.optimization_barrier(
        (feedforward_gate_weight, feedforward_up_weight, output_weight, state)
    )
    units = feedforward_gate_weight.shape[1]
    wide = -(-(units // 2 + 1) // 128) * 128
    packed = kernel_call(pack_kernel, shape(BF, 608, wide), count=4, name="pack")(
        gate_w, up_w, output_w, tokens
    )
    packed = lax.all_gather(packed, "core")
    got, state, packed = lax.optimization_barrier((got, state, packed))
    ready, own_value, outgate = kernel_call(
        query_kernel,
        (shape(F32, 16, 128), shape(F32, 1, DV), shape(F32, 1, DV)),
        scratch=[pltpu.VMEM((16, 128), F32)] * 2,
        count=3,
        name="query",
    )(got, decay_weight, bias)
    whole = lax.all_gather(ready, "core")
    part = kernel_call(heads_kernel, shape(F32, 32, DV), count=5, name="heads")(
        whole, near, state, own_value, outgate
    )
    second = kernel_call(
        sums_kernel,
        shape(BF, 16, HALF + 1, 2, 128),
        scratch=[pltpu.VMEM((32, DV), F32)],
        count=1,
        name="sums",
    )(lax.all_gather(part, "core"))
    back = exchange(second, Z)
    rows = kernel_call(
        gating_kernel,
        shape(BF, 32, 24, 128),
        scratch=[pltpu.VMEM((16, DV), F32)] * 2 + [pltpu.VMEM((24, 128), F32)],
        count=3,
        name="gating",
    )(back, head_norm_gain.reshape(1, DV), packed)
    rows = exchange(rows, ("core", *TP))
    third, residual = kernel_call(
        wide_kernel,
        (shape(BF, 16, OWN, 2, wide), shape(F32, 24, 128)),
        scratch=[pltpu.VMEM((2, 24, 128), F32)],
        count=3,
        name="wide",
    )(rows, feedforward_norm_gain.reshape(32, 128), packed)
    third = exchange(third, Z)
    hidden = kernel_call(
        hidden_kernel,
        shape(BF, 8, 8, wide),
        scratch=[pltpu.VMEM((8, wide), F32)] * 2,
        count=1,
        name="hidden",
    )(third)
    hidden = exchange(hidden, NEAR)
    down = kernel_call(
        down_kernel,
        shape(BF, 16, 24, 128),
        scratch=[pltpu.VMEM((24, wide), F32)],
        count=2,
        name="down",
    )(hidden, feedforward_down_weight)
    down = exchange(down, TP)
    return (residual + jnp.sum(down.astype(F32), axis=0)).astype(BF)


def solution(mesh):
    finer = Mesh(mesh.devices.reshape(4, 2, 2, 2, 4, 4), (*KV, *TP))
    placed = (
        P(None, KV),
        P(),
        P(KV, TP),
        P(KV, TP),
        P(KV, TP),
        P(KV, TP),
        P(),
        P(),
        P(),
        P(),
        P(TP, KV),
        P(),
        P(KV, TP),
        P(KV, TP),
        P(TP, KV),
        P(None, KV, TP),
        P(None, KV, TP),
        P(None, None, KV),
        P(None, TP, KV),
        P(),
    )
    return jax.shard_map(
        shards, mesh=finer, in_specs=placed, out_specs=P(None, KV), check_vma=False
    )
```

```python
import jax
import jax.numpy as jnp
from jax import lax
from jax.experimental import pallas as pl
from jax.experimental.pallas import tpu as pltpu
from jax.sharding import Mesh
from jax.sharding import PartitionSpec as P

D = 4096
KEY_CHANNELS = 128
DV = 256
GROUPS = 8
MEMBERS = 4
OWN = 6
Z = ("za", "zb", "zc")
KVL = ("zc", "core")
NEAR = ("zb", "zc", "core")
KV = (*Z, "core")
TP = ("tp_0", "tp_1")
NORM_EPSILON = 1e-06
BF = jnp.bfloat16
F32 = jnp.float32


BIG = 1e9
HALF = 12
VMEM_LIMIT = 16 * 1024 * 1024


def exchange(array, axes):
    return lax.all_to_all(array, axes, split_axis=0, concat_axis=0, tiled=True)


def copies(array, size):
    return jnp.broadcast_to(array, (size, *array.shape))


def iota(shape, dim):
    return lax.broadcasted_iota(jnp.int32, shape, dim)


def dot(lhs, rhs, contract=((1,), (0,))):
    return lax.dot_general(lhs, rhs, (contract, ((), ())), preferred_element_type=F32)


def rounded(array):
    return array.astype(BF).astype(F32)


def log_gate(values):
    return (jnp.minimum(values, 0.0) - jnp.log(1.0 + jnp.exp(-jnp.abs(values)))) * 0.0625


def silu(values):
    return values / (1.0 + jnp.exp(-values))


def place_of():
    group, member = lax.axis_index(("za", "zb")), lax.axis_index(KVL)
    return group, member, group * MEMBERS + member


def kernel_call(kernel, outs, scratch=(), hbm=(), flops=1_000_000, count=0, name=None):
    specs = [
        pl.BlockSpec(memory_space=pltpu.HBM if i in hbm else pltpu.VMEM) for i in range(count)
    ]
    many = isinstance(outs, (tuple, list))
    call = pl.pallas_call(
        kernel,
        out_shape=outs,
        in_specs=specs,
        out_specs=[pl.BlockSpec(memory_space=pltpu.VMEM)] * len(outs)
        if many
        else pl.BlockSpec(memory_space=pltpu.VMEM),
        scratch_shapes=list(scratch),
        cost_estimate=pl.CostEstimate(flops=flops, bytes_accessed=1_000_000, transcendentals=0),
        compiler_params=pltpu.CompilerParams(vmem_limit_bytes=VMEM_LIMIT),
        name=name,
    )
    return lambda *args: call(
        *(
            pltpu.with_memory_space_constraint(a, pltpu.HBM) if i in hbm else a
            for i, a in enumerate(args)
        )
    )


def fetched(pairs, sems):
    moves = [pltpu.make_async_copy(src, dst, sems.at[i]) for i, (src, dst) in enumerate(pairs)]
    for move in moves:
        move.start()
    return moves


def spread_rows(decay_cols):
    stacked = jnp.concatenate([decay_cols] * 8, axis=0)
    owner = lax.shift_right_logical(iota((128, 128), 0), 4)
    blocks = [jnp.where(owner == m, stacked, 0.0) for m in range(8)]
    seq_row = iota((16, 128), 0) & 7
    ones = [(seq_row == m).astype(F32) for m in range(8)]
    return jnp.concatenate(blocks, axis=1).astype(BF), jnp.concatenate(ones, axis=1).astype(BF)


def gate_inputs(b, lowcache, extra, blocks, ones, pre, add):
    pre[...] = dot(lowcache[128 * b : 128 * b + 128, :], blocks, ((0,), (0,)))
    lines = jnp.concatenate([extra[8 * b + m] for m in range(8)], axis=0)
    high = rounded(lines)
    both = jnp.concatenate([high, lines - high], axis=0).astype(BF)
    add[...] = dot(both, ones, ((0,), (0,)))


def start_kernel(
    lengths_h,
    lowcache_h,
    decay_h,
    bias_h,
    extra_h,
    tokens_h,
    gain_h,
    low_h,
    query_h,
    key_h,
    value_h,
    outgate_h,
    send,
    lengths,
    lowcache,
    decay,
    bias,
    extra,
    tokens,
    gain,
    low_w,
    query_w,
    key_w,
    value_w,
    outgate_w,
    pre,
    sems,
):
    group, member, place = place_of()
    head = lax.axis_index(TP)
    head_lanes = pl.ds(pl.multiple_of(head * 128, 128), 128)
    place_lanes = pl.ds(pl.multiple_of(place * 128, 128), 128)
    moves = fetched(
        [
            (decay_h.at[:, head_lanes], decay),
            (lowcache_h, lowcache),
            (extra_h, extra),
            (bias_h, bias),
            (lengths_h, lengths),
            (tokens_h, tokens),
            (gain_h, gain),
            (low_h.at[:, place_lanes], low_w),
            (query_h, query_w),
            (key_h, key_w),
            (value_h, value_w),
            (outgate_h, outgate_w),
        ],
        sems,
    )
    start = place * 192
    ids = start + iota((192, 128), 0)
    for move in moves[:5]:
        move.wait()
    blocks = spread_rows(decay[...].astype(F32))[0]
    bias_row = bias[pl.ds(head, 1), :]
    line_ids = start + iota((1, 192), 1)
    for b in range(3):
        pre[...] = dot(lowcache[128 * b : 128 * b + 128, :], blocks, ((0,), (0,)))
        for m in range(8):
            s, lanes = 8 * b + m, slice(128 * m, 128 * m + 128)
            value = jnp.where(ids < lengths[s], pre[:, lanes] + bias_row, BIG)
            factor = (1.0 + jnp.exp(-jnp.abs(value))).reshape(24, 8, 128)
            while factor.shape[0] > 3:
                half = factor.shape[0] // 2
                factor = factor[:half] * factor[half:]
            factor = factor[0] * factor[1] * factor[2]
            below = jnp.sum(jnp.minimum(value, 0.0).reshape(24, 8, 128), axis=0)
            gate = jnp.sum(below - jnp.log(factor), axis=0, keepdims=True) * 0.0625
            line = jnp.where(line_ids < lengths[s], extra[s], 0.0)
            send[24 + s : 25 + s, :] = gate + jnp.sum(line, axis=1, keepdims=True)
    for move in moves[5:]:
        move.wait()
    tokens_f = tokens[...].astype(F32)
    scaled = (tokens_f * gain[pl.ds(place, 1), :]).astype(BF)
    send[:24, :] = dot(scaled, query_w[...])
    send[48:72, :] = dot(scaled, key_w[...])
    for i, weights in enumerate((value_w, outgate_w)):
        out, at = dot(scaled, weights[...]), 72 + 48 * i
        send[at : at + 24, :] = out[:, :128]
        send[at + 24 : at + 48, :] = out[:, 128:]
    low_t = low_w[...].astype(F32)
    low_t = jnp.concatenate([low_t] * OWN + [jnp.zeros((32, 128), F32)], axis=0).astype(BF)
    low = dot(scaled, low_t, ((1,), (1,)))
    squares = jnp.sum(tokens_f * tokens_f, axis=1, keepdims=True)
    lane, row = iota((24, 128), 1), iota((24, 128), 0)
    owner = sum((row >= OWN * r).astype(jnp.int32) for r in range(1, MEMBERS))
    slot = row - OWN * owner
    line = jnp.where(lax.shift_right_logical(lane, 4) == slot, low, 0.0)
    line = jnp.where(lane >= 96, 0.0, line)
    line = jnp.where(lane == 96 + slot, squares, line)
    for r in range(MEMBERS):
        at = slice(OWN * r, OWN * r + OWN)
        send[168 + r : 169 + r, :] = jnp.sum(line[at], axis=0, keepdims=True)
    send[172:, :] = jnp.zeros((4, 128), F32)


def first_kernel(both, send, near, held, block):
    core = lax.axis_index("core")
    held[...] = both[0] + both[1]
    near[...] = jnp.zeros_like(near)
    for c in range(2):
        at = 24 + HALF * c
        near[c, :HALF, :] = jnp.where(core == 0, both[1, at : at + HALF, :], 0.0)

    def picked(start, size, step=HALF):
        low, high = held[start : start + size, :], held[start + step : start + step + size, :]
        return jnp.where(core == 0, low, high)

    lines = picked(168, 2, 2)
    lane = iota((2, 128), 1)
    is_square = (lane >= 96) & (lane < 102)
    top = jnp.where(is_square, rounded(lines), lines)
    rest = jnp.where(is_square, lines - rounded(lines), 0.0)
    block[...] = jnp.zeros_like(block)
    block[:HALF, :] = picked(0, HALF)
    block[HALF : 2 * HALF, :] = picked(24, HALF)
    block[24:26, :] = top + pltpu.roll(rest, OWN, 1)
    shared = block[:24, :].astype(BF)
    for z in range(16):
        s = min(z, HALF - 1)
        for a in range(5):
            block[26 + a : 27 + a, :] = picked(48 + 24 * a + s, 1)
        send[z, :24, :] = shared
        send[z, 24:, :] = block[24:, :].astype(BF)


def halves(row):
    return jnp.concatenate([row[:, :128], row[:, 128:]], axis=0).astype(BF)


def state_kernel(
    lengths_h,
    lowcache_h,
    decay_h,
    bias_h,
    extra_h,
    keys_h,
    values_h,
    state,
    lengths,
    lowcache,
    decay,
    bias,
    extra,
    keys,
    values,
    pre,
    add,
    rounded_gates,
    sems,
):
    _, _, place = place_of()
    head = lax.axis_index(TP)
    head_lanes = pl.ds(pl.multiple_of(head * 128, 128), 128)
    moves = fetched(
        [
            (decay_h.at[:, head_lanes], decay),
            (lowcache_h, lowcache),
            (extra_h, extra),
            (bias_h, bias),
            (lengths_h, lengths),
        ]
        + [
            (whole.at[8 * b : 8 * b + 8], part.at[8 * b : 8 * b + 8])
            for b in range(3)
            for whole, part in ((keys_h, keys), (values_h, values))
        ],
        sems,
    )
    later = (iota((192, 192), 1) > iota((192, 192), 0)).astype(F32).astype(BF)
    ids = place * 192 + iota((192, 128), 0)
    for move in moves[:5]:
        move.wait()
    blocks, ones = spread_rows(decay[...].astype(F32))
    bias_row = bias[pl.ds(head, 1), :]
    for b in range(3):
        gate_inputs(b, lowcache, extra, blocks, ones, pre, add)
        for m in range(8):
            lanes = slice(128 * m, 128 * m + 128)
            gate = log_gate(pre[:, lanes] + bias_row) + add[:, lanes]
            gate = jnp.where(ids < lengths[8 * b + m], gate, 0.0)
            rounded_gates[:, lanes] = gate.astype(BF)
        pre[...] = dot(later, rounded_gates[...])
        for move in moves[5 + 2 * b : 7 + 2 * b]:
            move.wait()
        for m in range(8):
            s, lanes = 8 * b + m, slice(128 * m, 128 * m + 128)
            weighted = keys[s].astype(F32) * jnp.exp(pre[:, lanes])
            weighted = jnp.where(ids < lengths[s], weighted, 0.0).astype(BF)
            state[128 * s : 128 * s + 128, :] = dot(weighted, values[s], ((0,), (0,))).astype(BF)


def query_kernel(
    got,
    decay_w,
    bias,
    ready,
    own_value,
    outgate,
    later,
    query_sum,
    sums,
    beyond_rows,
):
    _, _, place = place_of()
    level = lax.shift_right_logical(place, 1)
    head = lax.axis_index(TP)
    decay_cols = decay_w[:, pl.ds(pl.multiple_of(head * 128, 128), 128)].astype(F32)
    bias_row = bias[pl.ds(head, 1), :]
    stack = jnp.concatenate([decay_cols] * OWN + [jnp.zeros((32, 128), F32)], axis=0).astype(BF)

    sums[...] = jnp.sum(got[...].astype(F32), axis=0)
    beyond = jnp.zeros((24, 128), F32)
    for z in range(16):
        beyond = beyond + jnp.where(z > level, got[z, :24, :].astype(F32), 0.0)
    beyond_rows[...] = beyond
    later[...] = jnp.zeros_like(later)
    query_sum[...] = jnp.zeros_like(query_sum)
    later[:HALF, :] = beyond_rows[HALF:, :]
    query_sum[:HALF, :] = sums[:HALF, :]
    lines = sums[24:26, :]
    lane, row = iota((16, 128), 1), iota((16, 128), 0)
    wide = jnp.where(row < OWN, lines[0:1], lines[1:2])
    slot = jnp.where(row < OWN, row, row - OWN)
    held = row < HALF
    square = jnp.sum(
        jnp.where(held & ((lane == 96 + slot) | (lane == 102 + slot)), wide, 0.0),
        axis=1,
        keepdims=True,
    )
    inv = lax.rsqrt(square * (1.0 / D) + NORM_EPSILON)
    low = jnp.where((lax.shift_right_logical(lane, 4) == slot) & held, wide, 0.0)
    fresh = log_gate(dot((inv * low).astype(BF), stack) + bias_row)
    query = rounded(inv * query_sum[...]) * KEY_CHANNELS ** (-0.5)
    ready[...] = query * jnp.exp(fresh + later[...])
    is_own = row == level
    own_query = jnp.sum(jnp.where(is_own, query, 0.0), axis=0, keepdims=True)
    own_inv = jnp.sum(jnp.where(is_own[:, :1], inv, 0.0), axis=0, keepdims=True)
    key_new = rounded(own_inv * sums[26:27, :])
    own = jnp.sum(own_query * key_new, axis=1, keepdims=True)
    pair = own * rounded(own_inv * sums[27:29, :])
    own_value[:, :128], own_value[:, 128:] = pair[0:1], pair[1:2]
    pair = rounded(own_inv * sums[29:31, :])
    outgate[:, :128], outgate[:, 128:] = pair[0:1], pair[1:2]


def heads_kernel(whole, near, state, own_value, outgate, send):
    core = lax.axis_index("core")
    _, _, place = place_of()
    query = (whole[...] * jnp.exp(near[...])).reshape(32, 128)
    high = rounded(query)
    both = jnp.concatenate([high, query - high], axis=0)
    row = iota((64, 128), 0) & 31
    spread = jnp.concatenate(
        [
            jnp.where(row == 16 * (s // HALF) + s % HALF, both, 0.0).astype(BF)
            for s in range(24)
        ],
        axis=1,
    )
    part = dot(spread, state[...])
    part = part[:32] + part[32:]
    row = iota((32, DV), 0) - 16 * core
    part = part + jnp.where(row == lax.shift_right_logical(place, 1), own_value[...], 0.0)
    send[...] = jnp.where(row == HALF, outgate[...], part)


def sums_kernel(both, send, held):
    core = lax.axis_index("core")
    held[...] = both[0] + both[1]
    block = held[pl.ds(pl.multiple_of(16 * core, 16), 16), :]
    for k in range(HALF + 1):
        pair = halves(block[k : k + 1])
        for z in range(16):
            send[z, k] = pair


def gating_kernel(back, gain, packed, send, mixed_rows, gate_rows, held):
    mixed_rows[...] = jnp.zeros_like(mixed_rows)
    gate_rows[...] = jnp.zeros_like(gate_rows)
    for k in range(HALF):
        pair = jnp.sum(back[:, k].astype(F32), axis=0)
        mixed_rows[k : k + 1, :128], mixed_rows[k : k + 1, 128:] = pair[0:1], pair[1:2]
        pair = back[k, HALF].astype(F32)
        gate_rows[k : k + 1, :128], gate_rows[k : k + 1, 128:] = pair[0:1], pair[1:2]
    mixed = mixed_rows[...]
    mean_sq = jnp.sum(mixed * mixed, axis=1, keepdims=True) * (1.0 / DV)
    gated = mixed * lax.rsqrt(mean_sq + NORM_EPSILON) * gain[...] * silu(gate_rows[...])
    gated = gated.astype(BF)
    for c in range(2):
        weights = in_lanes(packed.at[c], 264, OUT_ROWS).astype(BF)
        held[HALF * c : HALF * c + HALF, :] = dot(gated, weights)[:HALF]
    rows = held[...].astype(BF)
    for h in range(32):
        send[h] = rows


OUT_ROWS = (56, 56, 56, 56, 32)


def pack_kernel(gate_w, up_w, output_w, tokens, send):
    half = gate_w.shape[1] // 2
    gate, up = gate_w[...].astype(F32), up_w[...].astype(F32)
    for c in range(2):
        lanes = slice(half * c, half * c + half)
        both = jnp.concatenate([gate[:, lanes], up[:, lanes]], axis=1)
        send[128 * c : 128 * c + 128, :] = both.astype(BF)
    send[256:, :] = jnp.zeros((send.shape[0] - 256, send.shape[1]), BF)
    for b in range(3):
        send[256:264, 128 * b : 128 * b + 128] = tokens[8 * b : 8 * b + 8, :]
    at = 0
    for b, size in enumerate(OUT_ROWS):
        send[264 : 264 + size, 128 * b : 128 * b + 128] = output_w[at : at + size, :]
        at += size


def in_lanes(packed, start, sizes):
    return jnp.concatenate(
        [
            packed[start : start + size, 128 * b : 128 * b + 128].astype(F32)
            for b, size in enumerate(sizes)
        ],
        axis=0,
    )


def wide_kernel(rows, gain, packed, send, residual, held, block):
    core = lax.axis_index("core")
    _, _, place = place_of()
    wide = square = 0.0
    for source in range(2):
        part = jnp.sum(rows[16 * source : 16 * source + 16].astype(F32), axis=0)
        for c in range(2):
            held[c, HALF * source : HALF * source + HALF, :] = part[HALF * c : HALF * c + HALF]
    for c in range(2):
        total = held[c] + in_lanes(packed.at[c], 256, (8, 8, 8))

        @pl.when(core == c)
        def _():
            residual[...] = total

        scaled = (total * gain[pl.ds(place - core + c, 1), :]).astype(BF)
        square += jnp.sum(total * total, axis=1, keepdims=True)
        wide += dot(scaled, packed[c, pl.ds(pl.multiple_of(128 * core, 128), 128), :])
    high = rounded(square)
    lane, row = iota((24, 128), 1), iota((24, 128), 0)
    slot = row - OWN * sum((row >= OWN * r).astype(jnp.int32) for r in range(1, MEMBERS))
    line = jnp.where(lane == slot, high, jnp.where(lane == OWN + slot, square - high, 0.0))
    tiles = wide.shape[1] // 128
    block[...] = jnp.zeros_like(block)
    for r in range(MEMBERS):
        for k in range(OWN):
            for t in range(tiles):
                at = tiles * k + t
                block[at : at + 1, :] = wide[OWN * r + k : OWN * r + k + 1, 128 * t : 128 * t + 128]
        at = tiles * OWN
        block[at : at + 1, :] = jnp.sum(line[OWN * r : OWN * r + OWN], axis=0, keepdims=True)
        whole = block[...].astype(BF)
        for z in range(4):
            send[4 * z + r] = whole


def hidden_kernel(got, send, held, sums):
    half = held.shape[1] // 2
    tiles = held.shape[1] // 128
    held[...] = jnp.zeros_like(held)
    sums[...] = jnp.sum(got[...].astype(F32), axis=0)
    for k in range(OWN):
        for t in range(tiles):
            at = tiles * k + t
            held[k : k + 1, 128 * t : 128 * t + 128] = sums[at : at + 1, :]
    line = jnp.broadcast_to(sums[tiles * OWN : tiles * OWN + 1, :], (8, 128))
    lane, row = iota((8, 128), 1), iota((8, 128), 0)
    own = (row < OWN) & ((lane == row) | (lane == OWN + row))
    square = jnp.sum(jnp.where(own, line, 0.0), axis=1, keepdims=True)
    inv = lax.rsqrt(square * (1.0 / D) + NORM_EPSILON)
    whole = held[...]
    hidden = silu(inv * whole[:, :half]) * (inv * whole[:, half:])
    zeros = jnp.zeros((8, send.shape[2] - half), F32)
    hidden = jnp.concatenate([hidden, zeros], axis=1).astype(BF)
    for j in range(8):
        send[j] = hidden


def down_kernel(got, down_w, send, held):
    half = down_w.shape[0] // 2
    total = 0.0
    for c in range(2):
        for z in range(4):
            held[OWN * z : OWN * z + OWN, :] = got[2 * z + c].astype(F32)[:OWN]
        total += dot(held[...].astype(BF)[:, :half], down_w[half * c : half * c + half, :])
    total = total.astype(BF)
    for h in range(16):
        send[h] = total


def shape(dtype, *dims):
    return jax.ShapeDtypeStruct(dims, dtype)


def shards(
    tokens,
    attention_norm_gain,
    query_weight,
    key_weight,
    value_weight,
    output_gate_weight,
    lowrank_weight,
    decay_weight,
    decay_preact_bias,
    head_norm_gain,
    output_weight,
    feedforward_norm_gain,
    feedforward_gate_weight,
    feedforward_up_weight,
    feedforward_down_weight,
    past_key_cache,
    past_value_cache,
    past_lowrank_cache,
    head_extra_decay,
    lengths,
):
    bias = decay_preact_bias.reshape(16, 128)
    lowcache = past_lowrank_cache.reshape(384, 192)
    gate_scratch = [
        pltpu.SMEM((24,), jnp.int32),
        pltpu.VMEM((384, 192), BF),
        pltpu.VMEM((16, 128), BF),
        pltpu.VMEM((16, 128), F32),
        pltpu.VMEM((24, 1, 192), F32),
    ]
    first = kernel_call(
        start_kernel,
        shape(F32, 176, 128),
        scratch=gate_scratch
        + [
            pltpu.VMEM((24, 128), BF),
            pltpu.VMEM((32, 128), F32),
            pltpu.VMEM((16, 128), BF),
            pltpu.VMEM((128, 128), BF),
            pltpu.VMEM((128, 128), BF),
            pltpu.VMEM((128, DV), BF),
            pltpu.VMEM((128, DV), BF),
            pltpu.VMEM((192, 1024), F32),
            pltpu.SemaphoreType.DMA((12,)),
        ],
        count=12,
        hbm=range(12),
        name="start",
    )(
        lengths,
        lowcache,
        decay_weight,
        bias,
        head_extra_decay,
        tokens,
        attention_norm_gain.reshape(32, 128),
        lowrank_weight.T,
        query_weight,
        key_weight,
        value_weight,
        output_gate_weight,
    )
    first, near = kernel_call(
        first_kernel,
        (shape(BF, 16, 32, 128), shape(F32, 2, 16, 128)),
        scratch=[pltpu.VMEM((176, 128), F32), pltpu.VMEM((32, 128), F32)],
        count=1,
        name="first",
    )(lax.all_gather(first, "core"))
    late_cache, first = lax.optimization_barrier((lowcache, first))
    got = exchange(first, Z)
    state = kernel_call(
        state_kernel,
        pltpu.VMEM((3072, DV), BF),
        scratch=gate_scratch
        + [
            pltpu.VMEM((24, 192, 128), BF),
            pltpu.VMEM((24, 192, DV), BF),
            pltpu.VMEM((192, 1024), F32),
            pltpu.VMEM((192, 1024), F32),
            pltpu.VMEM((192, 1024), BF),
            pltpu.SemaphoreType.DMA((11,)),
        ],
        count=7,
        hbm=range(7),
        flops=20_000_000_000,
        name="state",
    )(
        lengths,
        late_cache,
        decay_weight,
        bias,
        head_extra_decay,
        past_key_cache,
        past_value_cache,
    )
    gate_w, up_w, output_w, state = lax.optimization_barrier(
        (feedforward_gate_weight, feedforward_up_weight, output_weight, state)
    )
    units = feedforward_gate_weight.shape[1]
    wide = -(-units // 256) * 128
    lines = -(-(OWN * units // 128 + 1) // 16) * 16
    packed = kernel_call(pack_kernel, shape(BF, 320, units), count=4, name="pack")(
        gate_w, up_w, output_w, tokens
    )
    packed = lax.all_gather(packed, "core")
    got, state, packed = lax.optimization_barrier((got, state, packed))
    ready, own_value, outgate = kernel_call(
        query_kernel,
        (shape(F32, 16, 128), shape(F32, 1, DV), shape(F32, 1, DV)),
        scratch=[pltpu.VMEM((16, 128), F32)] * 2
        + [pltpu.VMEM((32, 128), F32), pltpu.VMEM((24, 128), F32)],
        count=3,
        name="query",
    )(got, decay_weight, bias)
    whole = lax.all_gather(ready, "core")
    part = kernel_call(heads_kernel, shape(F32, 32, DV), count=5, name="heads")(
        whole, near, state, own_value, outgate
    )
    second = kernel_call(
        sums_kernel,
        shape(BF, 16, HALF + 1, 2, 128),
        scratch=[pltpu.VMEM((32, DV), F32)],
        count=1,
        name="sums",
    )(lax.all_gather(part, "core"))
    back = exchange(second, Z)
    rows = kernel_call(
        gating_kernel,
        shape(BF, 32, 24, 128),
        scratch=[pltpu.VMEM((16, DV), F32)] * 2 + [pltpu.VMEM((24, 128), F32)],
        count=3,
        name="gating",
    )(back, head_norm_gain.reshape(1, DV), packed)
    rows = exchange(rows, ("core", *TP))
    third, residual = kernel_call(
        wide_kernel,
        (shape(BF, 16, lines, 128), shape(F32, 24, 128)),
        scratch=[pltpu.VMEM((2, 24, 128), F32), pltpu.VMEM((lines, 128), F32)],
        count=3,
        name="wide",
    )(rows, feedforward_norm_gain.reshape(32, 128), packed)
    third = exchange(third, Z)
    hidden = kernel_call(
        hidden_kernel,
        shape(BF, 8, 8, wide),
        scratch=[pltpu.VMEM((8, units), F32), pltpu.VMEM((lines, 128), F32)],
        count=1,
        name="hidden",
    )(third)
    hidden = exchange(hidden, NEAR)
    down = kernel_call(
        down_kernel,
        shape(BF, 16, 24, 128),
        scratch=[pltpu.VMEM((24, wide), F32)],
        count=2,
        name="down",
    )(hidden, feedforward_down_weight)
    down = exchange(down, TP)
    return (residual + jnp.sum(down.astype(F32), axis=0)).astype(BF)


def solution(mesh):
    finer = Mesh(mesh.devices.reshape(4, 2, 2, 2, 4, 4), (*KV, *TP))
    placed = (
        P(None, KV),
        P(),
        P(KV, TP),
        P(KV, TP),
        P(KV, TP),
        P(KV, TP),
        P(),
        P(),
        P(),
        P(),
        P(TP, KV),
        P(),
        P(KV, TP),
        P(KV, TP),
        P(TP, KV),
        P(None, KV, TP),
        P(None, KV, TP),
        P(None, None, KV),
        P(None, TP, KV),
        P(),
    )
    return jax.shard_map(
        shards, mesh=finer, in_specs=placed, out_specs=P(None, KV), check_vma=False
    )
```

```python
import jax
import jax.numpy as jnp
from jax import lax
from jax.experimental import pallas as pl
from jax.experimental.pallas import tpu as pltpu
from jax.sharding import Mesh
from jax.sharding import PartitionSpec as P

D = 4096
KEY_CHANNELS = 128
DV = 256
GROUPS = 8
MEMBERS = 4
OWN = 6
Z = ("za", "zb", "zc")
KVL = ("zc", "core")
NEAR = ("zb", "zc", "core")
KV = (*Z, "core")
TP = ("tp_0", "tp_1")
NORM_EPSILON = 1e-06
BF = jnp.bfloat16
F32 = jnp.float32


BIG = 1e9
HALF = 12
VMEM_LIMIT = 16 * 1024 * 1024


def exchange(array, axes):
    return lax.all_to_all(array, axes, split_axis=0, concat_axis=0, tiled=True)


def copies(array, size):
    return jnp.broadcast_to(array, (size, *array.shape))


def iota(shape, dim):
    return lax.broadcasted_iota(jnp.int32, shape, dim)


def dot(lhs, rhs, contract=((1,), (0,))):
    return lax.dot_general(lhs, rhs, (contract, ((), ())), preferred_element_type=F32)


def rounded(array):
    return array.astype(BF).astype(F32)


def log_gate(values):
    return (jnp.minimum(values, 0.0) - jnp.log(1.0 + jnp.exp(-jnp.abs(values)))) * 0.0625


def silu(values):
    return values / (1.0 + jnp.exp(-values))


def place_of():
    group, member = lax.axis_index(("za", "zb")), lax.axis_index(KVL)
    return group, member, group * MEMBERS + member


def kernel_call(kernel, outs, scratch=(), hbm=(), flops=1_000_000, count=0, name=None):
    specs = [
        pl.BlockSpec(memory_space=pltpu.HBM if i in hbm else pltpu.VMEM) for i in range(count)
    ]
    many = isinstance(outs, (tuple, list))
    call = pl.pallas_call(
        kernel,
        out_shape=outs,
        in_specs=specs,
        out_specs=[pl.BlockSpec(memory_space=pltpu.VMEM)] * len(outs)
        if many
        else pl.BlockSpec(memory_space=pltpu.VMEM),
        scratch_shapes=list(scratch),
        cost_estimate=pl.CostEstimate(flops=flops, bytes_accessed=1_000_000, transcendentals=0),
        compiler_params=pltpu.CompilerParams(vmem_limit_bytes=VMEM_LIMIT),
        name=name,
    )
    return lambda *args: call(
        *(
            pltpu.with_memory_space_constraint(a, pltpu.HBM) if i in hbm else a
            for i, a in enumerate(args)
        )
    )


def fetched(pairs, sems):
    moves = [pltpu.make_async_copy(src, dst, sems.at[i]) for i, (src, dst) in enumerate(pairs)]
    for move in moves:
        move.start()
    return moves


def spread_rows(decay_cols):
    stacked = jnp.concatenate([decay_cols] * 8, axis=0)
    owner = lax.shift_right_logical(iota((128, 128), 0), 4)
    blocks = [jnp.where(owner == m, stacked, 0.0) for m in range(8)]
    seq_row = iota((16, 128), 0) & 7
    ones = [(seq_row == m).astype(F32) for m in range(8)]
    return jnp.concatenate(blocks, axis=1).astype(BF), jnp.concatenate(ones, axis=1).astype(BF)


def gate_inputs(b, lowcache, extra, blocks, ones, pre, add):
    pre[...] = dot(lowcache[128 * b : 128 * b + 128, :], blocks, ((0,), (0,)))
    lines = jnp.concatenate([extra[8 * b + m] for m in range(8)], axis=0)
    high = rounded(lines)
    both = jnp.concatenate([high, lines - high], axis=0).astype(BF)
    add[...] = dot(both, ones, ((0,), (0,)))


def start_kernel(
    lengths_h,
    lowcache_h,
    decay_h,
    bias_h,
    extra_h,
    tokens_h,
    gain_h,
    low_h,
    query_h,
    key_h,
    value_h,
    outgate_h,
    send,
    lengths,
    lowcache,
    decay,
    bias,
    extra,
    tokens,
    gain,
    low_w,
    query_w,
    key_w,
    value_w,
    outgate_w,
    pre,
    sems,
):
    group, member, place = place_of()
    head = lax.axis_index(TP)
    head_lanes = pl.ds(pl.multiple_of(head * 128, 128), 128)
    place_lanes = pl.ds(pl.multiple_of(place * 128, 128), 128)
    moves = fetched(
        [
            (decay_h.at[:, head_lanes], decay),
            (lowcache_h, lowcache),
            (extra_h, extra),
            (bias_h, bias),
            (lengths_h, lengths),
            (tokens_h, tokens),
            (gain_h, gain),
            (low_h.at[:, place_lanes], low_w),
            (query_h, query_w),
            (key_h, key_w),
            (value_h, value_w),
            (outgate_h, outgate_w),
        ],
        sems,
    )
    start = place * 192
    ids = start + iota((192, 128), 0)
    for move in moves[:5]:
        move.wait()
    blocks = spread_rows(decay[...].astype(F32))[0]
    bias_row = bias[pl.ds(head, 1), :]
    line_ids = start + iota((1, 192), 1)
    for b in range(3):
        pre[...] = dot(lowcache[128 * b : 128 * b + 128, :], blocks, ((0,), (0,)))
        for m in range(8):
            s, lanes = 8 * b + m, slice(128 * m, 128 * m + 128)
            value = jnp.where(ids < lengths[s], pre[:, lanes] + bias_row, BIG)
            factor = (1.0 + jnp.exp(-jnp.abs(value))).reshape(24, 8, 128)
            while factor.shape[0] > 3:
                half = factor.shape[0] // 2
                factor = factor[:half] * factor[half:]
            factor = factor[0] * factor[1] * factor[2]
            below = jnp.sum(jnp.minimum(value, 0.0).reshape(24, 8, 128), axis=0)
            gate = jnp.sum(below - jnp.log(factor), axis=0, keepdims=True) * 0.0625
            line = jnp.where(line_ids < lengths[s], extra[s], 0.0)
            send[24 + s : 25 + s, :] = gate + jnp.sum(line, axis=1, keepdims=True)
    for move in moves[5:]:
        move.wait()
    tokens_f = tokens[...].astype(F32)
    scaled = (tokens_f * gain[pl.ds(place, 1), :]).astype(BF)
    send[:24, :] = dot(scaled, query_w[...])
    send[48:72, :] = dot(scaled, key_w[...])
    for i, weights in enumerate((value_w, outgate_w)):
        out, at = dot(scaled, weights[...]), 72 + 48 * i
        send[at : at + 24, :] = out[:, :128]
        send[at + 24 : at + 48, :] = out[:, 128:]
    low_t = low_w[...].astype(F32)
    low_t = jnp.concatenate([low_t] * OWN + [jnp.zeros((32, 128), F32)], axis=0).astype(BF)
    low = dot(scaled, low_t, ((1,), (1,)))
    squares = jnp.sum(tokens_f * tokens_f, axis=1, keepdims=True)
    lane, row = iota((24, 128), 1), iota((24, 128), 0)
    owner = sum((row >= OWN * r).astype(jnp.int32) for r in range(1, MEMBERS))
    slot = row - OWN * owner
    line = jnp.where(lax.shift_right_logical(lane, 4) == slot, low, 0.0)
    line = jnp.where(lane >= 96, 0.0, line)
    line = jnp.where(lane == 96 + slot, squares, line)
    for r in range(MEMBERS):
        at = slice(OWN * r, OWN * r + OWN)
        send[168 + r : 169 + r, :] = jnp.sum(line[at], axis=0, keepdims=True)
    send[172:, :] = jnp.zeros((4, 128), F32)


def first_kernel(both, send, near, held, block):
    core = lax.axis_index("core")
    held[...] = both[0] + both[1]
    near[...] = jnp.zeros_like(near)
    for c in range(2):
        at = 24 + HALF * c
        near[c, :HALF, :] = jnp.where(core == 0, both[1, at : at + HALF, :], 0.0)

    def picked(start, size, step=HALF):
        low, high = held[start : start + size, :], held[start + step : start + step + size, :]
        return jnp.where(core == 0, low, high)

    lines = picked(168, 2, 2)
    lane = iota((2, 128), 1)
    is_square = (lane >= 96) & (lane < 102)
    top = jnp.where(is_square, rounded(lines), lines)
    rest = jnp.where(is_square, lines - rounded(lines), 0.0)
    block[...] = jnp.zeros_like(block)
    block[:HALF, :] = picked(0, HALF)
    block[HALF : 2 * HALF, :] = picked(24, HALF)
    block[24:26, :] = top + pltpu.roll(rest, OWN, 1)
    shared = block[:24, :].astype(BF)
    for z in range(16):
        s = min(z, HALF - 1)
        for a in range(5):
            block[26 + a : 27 + a, :] = picked(48 + 24 * a + s, 1)
        send[z, :24, :] = shared
        send[z, 24:, :] = block[24:, :].astype(BF)


def halves(row):
    return jnp.concatenate([row[:, :128], row[:, 128:]], axis=0).astype(BF)


def state_kernel(
    lengths_h,
    lowcache_h,
    decay_h,
    bias_h,
    extra_h,
    keys_h,
    values_h,
    state,
    lengths,
    lowcache,
    decay,
    bias,
    extra,
    keys,
    values,
    pre,
    add,
    rounded_gates,
    sems,
):
    _, _, place = place_of()
    head = lax.axis_index(TP)
    head_lanes = pl.ds(pl.multiple_of(head * 128, 128), 128)
    moves = fetched(
        [
            (decay_h.at[:, head_lanes], decay),
            (lowcache_h, lowcache),
            (extra_h, extra),
            (bias_h, bias),
            (lengths_h, lengths),
        ]
        + [
            (whole.at[8 * b : 8 * b + 8], part.at[8 * b : 8 * b + 8])
            for b in range(3)
            for whole, part in ((keys_h, keys), (values_h, values))
        ],
        sems,
    )
    later = (iota((192, 192), 1) > iota((192, 192), 0)).astype(F32).astype(BF)
    ids = place * 192 + iota((192, 128), 0)
    for move in moves[:5]:
        move.wait()
    blocks, ones = spread_rows(decay[...].astype(F32))
    bias_row = bias[pl.ds(head, 1), :]
    for b in range(3):
        gate_inputs(b, lowcache, extra, blocks, ones, pre, add)
        for m in range(8):
            lanes = slice(128 * m, 128 * m + 128)
            gate = log_gate(pre[:, lanes] + bias_row) + add[:, lanes]
            gate = jnp.where(ids < lengths[8 * b + m], gate, 0.0)
            rounded_gates[:, lanes] = gate.astype(BF)
        pre[...] = dot(later, rounded_gates[...])
        for move in moves[5 + 2 * b : 7 + 2 * b]:
            move.wait()
        for m in range(8):
            s, lanes = 8 * b + m, slice(128 * m, 128 * m + 128)
            weighted = keys[s].astype(F32) * jnp.exp(pre[:, lanes])
            weighted = jnp.where(ids < lengths[s], weighted, 0.0).astype(BF)
            state[128 * s : 128 * s + 128, :] = dot(weighted, values[s], ((0,), (0,))).astype(BF)


def query_kernel(
    got,
    decay_w,
    bias,
    ready,
    own_value,
    outgate,
    later,
    query_sum,
    sums,
    beyond_rows,
):
    _, _, place = place_of()
    level = lax.shift_right_logical(place, 1)
    head = lax.axis_index(TP)
    decay_cols = decay_w[:, pl.ds(pl.multiple_of(head * 128, 128), 128)].astype(F32)
    bias_row = bias[pl.ds(head, 1), :]
    stack = jnp.concatenate([decay_cols] * OWN + [jnp.zeros((32, 128), F32)], axis=0).astype(BF)

    sums[...] = jnp.sum(got[...].astype(F32), axis=0)
    beyond = jnp.zeros((24, 128), F32)
    for z in range(16):
        beyond = beyond + jnp.where(z > level, got[z, :24, :].astype(F32), 0.0)
    beyond_rows[...] = beyond
    later[...] = jnp.zeros_like(later)
    query_sum[...] = jnp.zeros_like(query_sum)
    later[:HALF, :] = beyond_rows[HALF:, :]
    query_sum[:HALF, :] = sums[:HALF, :]
    lines = sums[24:26, :]
    lane, row = iota((16, 128), 1), iota((16, 128), 0)
    wide = jnp.where(row < OWN, lines[0:1], lines[1:2])
    slot = jnp.where(row < OWN, row, row - OWN)
    held = row < HALF
    square = jnp.sum(
        jnp.where(held & ((lane == 96 + slot) | (lane == 102 + slot)), wide, 0.0),
        axis=1,
        keepdims=True,
    )
    inv = lax.rsqrt(square * (1.0 / D) + NORM_EPSILON)
    low = jnp.where((lax.shift_right_logical(lane, 4) == slot) & held, wide, 0.0)
    fresh = log_gate(dot((inv * low).astype(BF), stack) + bias_row)
    query = rounded(inv * query_sum[...]) * KEY_CHANNELS ** (-0.5)
    ready[...] = query * jnp.exp(fresh + later[...])
    is_own = row == level
    own_query = jnp.sum(jnp.where(is_own, query, 0.0), axis=0, keepdims=True)
    own_inv = jnp.sum(jnp.where(is_own[:, :1], inv, 0.0), axis=0, keepdims=True)
    key_new = rounded(own_inv * sums[26:27, :])
    own = jnp.sum(own_query * key_new, axis=1, keepdims=True)
    pair = own * rounded(own_inv * sums[27:29, :])
    own_value[:, :128], own_value[:, 128:] = pair[0:1], pair[1:2]
    pair = rounded(own_inv * sums[29:31, :])
    outgate[:, :128], outgate[:, 128:] = pair[0:1], pair[1:2]


def heads_kernel(whole, near, state, own_value, outgate, send):
    core = lax.axis_index("core")
    _, _, place = place_of()
    query = (whole[...] * jnp.exp(near[...])).reshape(32, 128)
    high = rounded(query)
    both = jnp.concatenate([high, query - high], axis=0)
    row = iota((64, 128), 0) & 31
    spread = jnp.concatenate(
        [
            jnp.where(row == 16 * (s // HALF) + s % HALF, both, 0.0).astype(BF)
            for s in range(24)
        ],
        axis=1,
    )
    part = dot(spread, state[...])
    part = part[:32] + part[32:]
    row = iota((32, DV), 0) - 16 * core
    part = part + jnp.where(row == lax.shift_right_logical(place, 1), own_value[...], 0.0)
    send[...] = jnp.where(row == HALF, outgate[...], part)


def sums_kernel(both, send, held):
    core = lax.axis_index("core")
    held[...] = both[0] + both[1]
    block = held[pl.ds(pl.multiple_of(16 * core, 16), 16), :]
    for k in range(HALF + 1):
        pair = halves(block[k : k + 1])
        for z in range(16):
            send[z, k] = pair


def gating_kernel(back, gain, packed, send, mixed_rows, gate_rows, held):
    mixed_rows[...] = jnp.zeros_like(mixed_rows)
    gate_rows[...] = jnp.zeros_like(gate_rows)
    for k in range(HALF):
        pair = jnp.sum(back[:, k].astype(F32), axis=0)
        mixed_rows[k : k + 1, :128], mixed_rows[k : k + 1, 128:] = pair[0:1], pair[1:2]
        pair = back[k, HALF].astype(F32)
        gate_rows[k : k + 1, :128], gate_rows[k : k + 1, 128:] = pair[0:1], pair[1:2]
    mixed = mixed_rows[...]
    mean_sq = jnp.sum(mixed * mixed, axis=1, keepdims=True) * (1.0 / DV)
    gated = mixed * lax.rsqrt(mean_sq + NORM_EPSILON) * gain[...] * silu(gate_rows[...])
    gated = gated.astype(BF)
    for c in range(2):
        weights = in_lanes(packed.at[c], 264, OUT_ROWS).astype(BF)
        held[HALF * c : HALF * c + HALF, :] = dot(gated, weights)[:HALF]
    rows = held[...].astype(BF)
    for h in range(32):
        send[h] = rows


OUT_ROWS = (56, 56, 56, 56, 32)


def pack_kernel(gate_w, up_w, output_w, tokens, send):
    half = gate_w.shape[1] // 2
    gate, up = gate_w[...].astype(F32), up_w[...].astype(F32)
    for c in range(2):
        lanes = slice(half * c, half * c + half)
        both = jnp.concatenate([gate[:, lanes], up[:, lanes]], axis=1)
        send[128 * c : 128 * c + 128, :] = both.astype(BF)
    send[256:, :] = jnp.zeros((send.shape[0] - 256, send.shape[1]), BF)
    for b in range(3):
        send[256:264, 128 * b : 128 * b + 128] = tokens[8 * b : 8 * b + 8, :]
    at = 0
    for b, size in enumerate(OUT_ROWS):
        send[264 : 264 + size, 128 * b : 128 * b + 128] = output_w[at : at + size, :]
        at += size


def in_lanes(packed, start, sizes):
    return jnp.concatenate(
        [
            packed[start : start + size, 128 * b : 128 * b + 128].astype(F32)
            for b, size in enumerate(sizes)
        ],
        axis=0,
    )


def wide_kernel(rows, gain, packed, send, residual, held, block):
    core = lax.axis_index("core")
    _, _, place = place_of()
    wide = square = 0.0
    for source in range(2):
        part = jnp.sum(rows[16 * source : 16 * source + 16].astype(F32), axis=0)
        for c in range(2):
            held[c, HALF * source : HALF * source + HALF, :] = part[HALF * c : HALF * c + HALF]
    for c in range(2):
        total = held[c] + in_lanes(packed.at[c], 256, (8, 8, 8))

        @pl.when(core == c)
        def _():
            residual[...] = total

        scaled = (total * gain[pl.ds(place - core + c, 1), :]).astype(BF)
        square += jnp.sum(total * total, axis=1, keepdims=True)
        wide += dot(scaled, packed[c, pl.ds(pl.multiple_of(128 * core, 128), 128), :])
    high = rounded(square)
    lane, row = iota((24, 128), 1), iota((24, 128), 0)
    slot = row - HALF * (row >= HALF).astype(jnp.int32)
    line = jnp.where(lane == slot, high, jnp.where(lane == HALF + slot, square - high, 0.0))
    tiles = wide.shape[1] // 128
    block[...] = jnp.zeros_like(block)
    for r in range(2):
        for k in range(HALF):
            for t in range(tiles):
                at = tiles * k + t
                block[at : at + 1, :] = wide[HALF * r + k : HALF * r + k + 1, 128 * t : 128 * t + 128]
        at = tiles * HALF
        block[at : at + 1, :] = jnp.sum(line[HALF * r : HALF * r + HALF], axis=0, keepdims=True)
        whole = block[...].astype(BF)
        for z in range(8):
            send[2 * z + r] = whole


def hidden_kernel(got, send, held, sums):
    half = held.shape[1] // 2
    tiles = held.shape[1] // 128
    held[...] = jnp.zeros_like(held)
    sums[...] = jnp.sum(got[...].astype(F32), axis=0)
    for k in range(HALF):
        for t in range(tiles):
            at = tiles * k + t
            held[k : k + 1, 128 * t : 128 * t + 128] = sums[at : at + 1, :]
    line = jnp.broadcast_to(sums[tiles * HALF : tiles * HALF + 1, :], (16, 128))
    lane, row = iota((16, 128), 1), iota((16, 128), 0)
    own = (row < HALF) & ((lane == row) | (lane == HALF + row))
    square = jnp.sum(jnp.where(own, line, 0.0), axis=1, keepdims=True)
    inv = lax.rsqrt(square * (1.0 / D) + NORM_EPSILON)
    whole = held[...]
    hidden = silu(inv * whole[:, :half]) * (inv * whole[:, half:])
    zeros = jnp.zeros((16, send.shape[2] - half), F32)
    hidden = jnp.concatenate([hidden, zeros], axis=1).astype(BF)
    for j in range(4):
        send[j] = hidden


def down_kernel(got, down_w, send, held):
    half = down_w.shape[0] // 2
    total = 0.0
    for c in range(2):
        for z in range(2):
            held[HALF * z : HALF * z + HALF, :] = got[2 * z + c].astype(F32)[:HALF]
        total += dot(held[...].astype(BF)[:, :half], down_w[half * c : half * c + half, :])
    total = total.astype(BF)
    for h in range(16):
        send[h] = total


def shape(dtype, *dims):
    return jax.ShapeDtypeStruct(dims, dtype)


def shards(
    tokens,
    attention_norm_gain,
    query_weight,
    key_weight,
    value_weight,
    output_gate_weight,
    lowrank_weight,
    decay_weight,
    decay_preact_bias,
    head_norm_gain,
    output_weight,
    feedforward_norm_gain,
    feedforward_gate_weight,
    feedforward_up_weight,
    feedforward_down_weight,
    past_key_cache,
    past_value_cache,
    past_lowrank_cache,
    head_extra_decay,
    lengths,
):
    bias = decay_preact_bias.reshape(16, 128)
    lowcache = past_lowrank_cache.reshape(384, 192)
    gate_scratch = [
        pltpu.SMEM((24,), jnp.int32),
        pltpu.VMEM((384, 192), BF),
        pltpu.VMEM((16, 128), BF),
        pltpu.VMEM((16, 128), F32),
        pltpu.VMEM((24, 1, 192), F32),
    ]
    first = kernel_call(
        start_kernel,
        shape(F32, 176, 128),
        scratch=gate_scratch
        + [
            pltpu.VMEM((24, 128), BF),
            pltpu.VMEM((32, 128), F32),
            pltpu.VMEM((16, 128), BF),
            pltpu.VMEM((128, 128), BF),
            pltpu.VMEM((128, 128), BF),
            pltpu.VMEM((128, DV), BF),
            pltpu.VMEM((128, DV), BF),
            pltpu.VMEM((192, 1024), F32),
            pltpu.SemaphoreType.DMA((12,)),
        ],
        count=12,
        hbm=range(12),
        name="start",
    )(
        lengths,
        lowcache,
        decay_weight,
        bias,
        head_extra_decay,
        tokens,
        attention_norm_gain.reshape(32, 128),
        lowrank_weight.T,
        query_weight,
        key_weight,
        value_weight,
        output_gate_weight,
    )
    first, near = kernel_call(
        first_kernel,
        (shape(BF, 16, 32, 128), shape(F32, 2, 16, 128)),
        scratch=[pltpu.VMEM((176, 128), F32), pltpu.VMEM((32, 128), F32)],
        count=1,
        name="first",
    )(lax.all_gather(first, "core"))
    late_cache, first = lax.optimization_barrier((lowcache, first))
    got = exchange(first, Z)
    state = kernel_call(
        state_kernel,
        pltpu.VMEM((3072, DV), BF),
        scratch=gate_scratch
        + [
            pltpu.VMEM((24, 192, 128), BF),
            pltpu.VMEM((24, 192, DV), BF),
            pltpu.VMEM((192, 1024), F32),
            pltpu.VMEM((192, 1024), F32),
            pltpu.VMEM((192, 1024), BF),
            pltpu.SemaphoreType.DMA((11,)),
        ],
        count=7,
        hbm=range(7),
        flops=20_000_000_000,
        name="state",
    )(
        lengths,
        late_cache,
        decay_weight,
        bias,
        head_extra_decay,
        past_key_cache,
        past_value_cache,
    )
    gate_w, up_w, output_w, state = lax.optimization_barrier(
        (feedforward_gate_weight, feedforward_up_weight, output_weight, state)
    )
    units = feedforward_gate_weight.shape[1]
    wide = -(-units // 256) * 128
    lines = -(-(HALF * units // 128 + 1) // 16) * 16
    packed = kernel_call(pack_kernel, shape(BF, 320, units), count=4, name="pack")(
        gate_w, up_w, output_w, tokens
    )
    packed = lax.all_gather(packed, "core")
    got, state, packed = lax.optimization_barrier((got, state, packed))
    ready, own_value, outgate = kernel_call(
        query_kernel,
        (shape(F32, 16, 128), shape(F32, 1, DV), shape(F32, 1, DV)),
        scratch=[pltpu.VMEM((16, 128), F32)] * 2
        + [pltpu.VMEM((32, 128), F32), pltpu.VMEM((24, 128), F32)],
        count=3,
        name="query",
    )(got, decay_weight, bias)
    whole = lax.all_gather(ready, "core")
    part = kernel_call(heads_kernel, shape(F32, 32, DV), count=5, name="heads")(
        whole, near, state, own_value, outgate
    )
    second = kernel_call(
        sums_kernel,
        shape(BF, 16, HALF + 1, 2, 128),
        scratch=[pltpu.VMEM((32, DV), F32)],
        count=1,
        name="sums",
    )(lax.all_gather(part, "core"))
    back = exchange(second, Z)
    rows = kernel_call(
        gating_kernel,
        shape(BF, 32, 24, 128),
        scratch=[pltpu.VMEM((16, DV), F32)] * 2 + [pltpu.VMEM((24, 128), F32)],
        count=3,
        name="gating",
    )(back, head_norm_gain.reshape(1, DV), packed)
    rows = exchange(rows, ("core", *TP))
    third, residual = kernel_call(
        wide_kernel,
        (shape(BF, 16, lines, 128), shape(F32, 24, 128)),
        scratch=[pltpu.VMEM((2, 24, 128), F32), pltpu.VMEM((lines, 128), F32)],
        count=3,
        name="wide",
    )(rows, feedforward_norm_gain.reshape(32, 128), packed)
    third = exchange(third, Z)
    hidden = kernel_call(
        hidden_kernel,
        shape(BF, 4, 16, wide),
        scratch=[pltpu.VMEM((16, units), F32), pltpu.VMEM((lines, 128), F32)],
        count=1,
        name="hidden",
    )(third)
    hidden = exchange(hidden, KVL)
    down = kernel_call(
        down_kernel,
        shape(BF, 16, 24, 128),
        scratch=[pltpu.VMEM((24, wide), F32)],
        count=2,
        name="down",
    )(hidden, feedforward_down_weight)
    down = exchange(down, TP)
    return (residual + jnp.sum(down.astype(F32), axis=0)).astype(BF)


def solution(mesh):
    finer = Mesh(mesh.devices.reshape(4, 2, 2, 2, 4, 4), (*KV, *TP))
    placed = (
        P(None, KV),
        P(),
        P(KV, TP),
        P(KV, TP),
        P(KV, TP),
        P(KV, TP),
        P(),
        P(),
        P(),
        P(),
        P(TP, KV),
        P(),
        P(KV, TP),
        P(KV, TP),
        P(TP, KV),
        P(None, KV, TP),
        P(None, KV, TP),
        P(None, None, KV),
        P(None, TP, KV),
        P(),
    )
    return jax.shard_map(
        shards, mesh=finer, in_specs=placed, out_specs=P(None, KV), check_vma=False
    )
```
